32 devices in a mesh: grp: 2 (over y), fs: 4 (over z), tp: 4 (over x, core).
Axes of the slice: x: 2, y: 2, z: 4, core: 2. Of those that a mesh axis runs over, the one named last changes fastest.
Arguments:
- tokens: bfloat16 [32, 128, 2048], P(('grp', 'fs'), None, 'tp'), parts along dimension 0, may hold values from -100 to 100
- mix_gain: float32 [2048], replicated, may hold values from 0.1 to 1.9
- gate_outer: bfloat16 [2048, 1024], P('fs', 'tp'), may hold values from -0.125 to 0.125
- gate_inner: bfloat16 [2048, 1024], P('fs', 'tp'), may hold values from -0.125 to 0.125
- value_weight: bfloat16 [2048, 1024], P('fs', 'tp'), may hold values from -0.125 to 0.125
- conv_taps: float32 [3, 1024], replicated, may hold values from -3 to 3
- mix_out: bfloat16 [1024, 2048], P('tp', 'fs'), may hold values from -0.25 to 0.25
- ffn_gain: float32 [2048], replicated, may hold values from 0.1 to 1.9
- ffn_gate: bfloat16 [2048, 5632], P('fs', 'tp'), may hold values from -0.125 to 0.125
- ffn_up: bfloat16 [2048, 5632], P('fs', 'tp'), may hold values from -0.125 to 0.125
- ffn_down: bfloat16 [5632, 2048], P('tp', 'fs'), may hold values from -0.109375 to 0.109375
- out_gain: float32 [2048], replicated, may hold values from 0.1 to 1.9
Outputs:
- layer_out: bfloat16 [32, 128, 2048], P(('grp', 'fs'), None, 'tp'), parts along dimension 0
The draws below stay inside these ranges and needn't reach their ends.
There are 2 independent parts, one for each index of `grp`. The reference program is written for one: setup_inputs(seed, part) draws one part's arguments, and reference() takes and returns one part's arrays. A program takes and returns all parts, laid end to end along the dimension named above; an argument that names none is the same for every part. Nothing has to cross between parts.
All inputs are finite; a program needn't handle non-finite values.
Results may differ from the reference program's by a relative error of at most 0.015.
Values may be sent and summed in bfloat16 or wider, within the bound.
A program may use at most 64 MiB of HBM per device.

```python
import math
import jax
import jax.numpy as jnp
from jax import lax

D = 2048
CA = 1024
FF = 5632
TAPS = 3
LEN = 128
SEQS = 16
N_TP = 4


def draw_tokens(key, part):
    first_key, second_key = jax.random.split(jax.random.fold_in(key, 11), 2)
    ramp = jnp.exp(jnp.linspace(math.log(0.4), math.log(4.0), D)).astype(jnp.float32)
    rough = jax.random.uniform(second_key, (D,), jnp.float32, 0.6, 1.4)
    values = jax.random.normal(first_key, (SEQS, LEN, D), jnp.float32) * ramp * rough
    return jnp.clip(values, -100.0, 100.0).astype(jnp.bfloat16)


def with_spikes(drawn, own_key, source, target, parts, factor):
    owner, partner = [(jnp.arange(drawn.shape[dim]) // (drawn.shape[dim] // parts)).reshape([-1 if axis == dim else 1 for axis in range(drawn.ndim)]) for dim in (source, target)]
    chosen = jax.random.permutation(own_key, parts)[partner]
    strong = (owner == chosen) | (owner == (partner + parts // 2) % parts)
    return jnp.where(strong, factor * drawn, drawn)


def block_levels(stream_key, dims, cuts, low, largest):
    factor_of, own = 1.0, jax.random.fold_in(stream_key, 6)
    for axis_at, shards_of in cuts:
        draws = jnp.exp(jax.random.uniform(jax.random.fold_in(own, axis_at), (shards_of,), jnp.float32, low / len(cuts), largest / len(cuts)))
        factor_of = factor_of * jnp.repeat(draws, dims[axis_at] // shards_of).reshape([-1 if axis == axis_at else 1 for axis in range(len(dims))])
    return factor_of


def centred(own_key, dims, spread, limit, cuts=(), held_as=jnp.bfloat16):
    values = spread * jax.random.normal(own_key, dims, jnp.float32)
    if cuts:
        values = values * block_levels(own_key, dims, cuts, -0.22, 0.18)
    return jnp.clip(values, -limit, limit).astype(held_as)


def gaussian_with(key, extent, scale, limit, pieces, heavy, held_as=jnp.bfloat16):
    result = scale * jax.random.normal(key, extent, jnp.float32)
    if pieces:
        result = result * block_levels(key, extent, pieces, -0.22, 0.18)
    return jnp.clip(with_spikes(result, jax.random.fold_in(key, 3), *heavy), -limit, limit).astype(held_as)


def setup_inputs(seed: int = 0, part: int = 0) -> dict:
    streams_of = jax.random.split(jax.random.key(seed), 13)
    part_splits = jax.random.split(jax.random.fold_in(streams_of[12], part), 13)
    return {
        "tokens": draw_tokens(jax.random.fold_in(jax.random.fold_in(streams_of[12], part), 71), part),
        "mix_gain": jnp.clip(1.0 + 0.18 * jax.random.normal(streams_of[1], (D,), jnp.float32), 0.1, 1.9),
        "gate_outer": centred(streams_of[2], (D, CA), D ** -0.5, 0.125, ((0, 4), (1, 4))),
        "gate_inner": centred(streams_of[3], (D, CA), D ** -0.5, 0.125, ((0, 4), (1, 4))),
        "value_weight": centred(streams_of[4], (D, CA), D ** -0.5, 0.125, ((0, 4), (1, 4))),
        "conv_taps": centred(streams_of[5], (TAPS, CA), 0.6, 3.0, (), jnp.float32),
        "mix_out": gaussian_with(streams_of[6], (CA, D), CA ** -0.5, 0.25, ((0, 4), (1, 4)), (0, 1, 4, 2.0)),
        "ffn_gain": jnp.clip(1.0 + 0.18 * jax.random.normal(streams_of[7], (D,), jnp.float32), 0.1, 1.9),
        "ffn_gate": centred(streams_of[8], (D, FF), D ** -0.5, 0.125, ((0, 4), (1, 4))),
        "ffn_up": centred(streams_of[9], (D, FF), D ** -0.5, 0.125, ((0, 4), (1, 4))),
        "ffn_down": gaussian_with(streams_of[10], (FF, D), FF ** -0.5, 0.109375, ((0, 4), (1, 4)), (0, 1, 4, 2.0)),
        "out_gain": jnp.clip(1.0 + 0.18 * jax.random.normal(streams_of[11], (D,), jnp.float32), 0.1, 1.9),
    }


def rms_norm(values, gain):
    floats = values.astype(jnp.float32)
    scaled = floats * lax.rsqrt(lax.optimization_barrier(jnp.mean(floats * floats, axis=-1, keepdims=True)) + 1e-06)
    return scaled * gain.astype(jnp.float32)

def blocked_sum(left, weight, blocks):
    width = left.shape[1] // blocks
    summed = jnp.zeros((left.shape[0], weight.shape[1]), jnp.float32)
    for number in range(blocks):
        partial_value = jnp.dot(left[:, number * width:(number + 1) * width], weight[number * width:(number + 1) * width], preferred_element_type=jnp.float32).astype(jnp.bfloat16)
        summed = summed + lax.optimization_barrier(partial_value).astype(jnp.float32)
    return summed

def reference(tokens, mix_gain, gate_outer, gate_inner, value_weight, conv_taps, mix_out, ffn_gain, ffn_gate, ffn_up, ffn_down, out_gain):
    rows = SEQS * LEN
    flat = tokens.reshape(rows, D)
    normed = rms_norm(flat, mix_gain).astype(jnp.bfloat16)
    outer = jnp.dot(normed, gate_outer, preferred_element_type=jnp.float32).astype(jnp.bfloat16)
    inner = jnp.dot(normed, gate_inner, preferred_element_type=jnp.float32).astype(jnp.bfloat16)
    values = jnp.dot(normed, value_weight, preferred_element_type=jnp.float32).astype(jnp.bfloat16)
    product = (inner.astype(jnp.float32) * values.astype(jnp.float32)).reshape(SEQS, LEN, CA)
    padded = jnp.pad(product, ((0, 0), (TAPS - 1, 0), (0, 0)))
    conv = jnp.zeros((SEQS, LEN, CA), jnp.float32)
    for offset in range(TAPS):
        conv = conv + conv_taps[offset].astype(jnp.float32) * padded[:, offset:offset + LEN]
    gated = (outer.astype(jnp.float32) * conv.reshape(rows, CA)).astype(jnp.bfloat16)
    first = (flat.astype(jnp.float32) + blocked_sum(gated, mix_out, N_TP)).astype(jnp.bfloat16)
    normed_ffn = rms_norm(first, ffn_gain).astype(jnp.bfloat16)
    gate = jnp.dot(normed_ffn, ffn_gate, preferred_element_type=jnp.float32)
    upward = jnp.dot(normed_ffn, ffn_up, preferred_element_type=jnp.float32)
    hidden = (jax.nn.silu(gate) * upward).astype(jnp.bfloat16)
    second = first.astype(jnp.float32) + blocked_sum(hidden, ffn_down, N_TP)
    return rms_norm(second, out_gain).astype(jnp.bfloat16).reshape(SEQS, LEN, D)
```

```python
import functools

import jax
import jax.numpy as jnp
from jax import lax
from jax.experimental import pallas as pl
from jax.experimental.pallas import tpu as pltpu
from jax.sharding import PartitionSpec as P

MESH = pl.DeviceIdType.MESH
F32 = jnp.float32
BF16 = jnp.bfloat16
MIXER = 4
GATE, UP, DOWN = 4, 5, 6


def chunks_of(half):
    return next(count for count in (4, 2, 1) if half % (count * 16) == 0 or count == 1)


def column(rows):
    wide = jnp.broadcast_to(rows, (rows.shape[1], rows.shape[1]))
    return jnp.transpose(wide)[:, :1]


def kernel(
    n, parts, n_tp, length, chunk_counts,
    tok_ref, mix_gain, w0, w1, w2, taps_ref, w3, ffn_gain, w4, w5, w6, out_gain,
    out_ref,
    f0, f1, f2, f3, f4, f5, f6,
    tok_full, normed, proj, gated, mix_part, mix_recv, first_full, hidden, down_part, down_recv, sq_send, sq_recv,
    right_send, left_send, z_recv, y_send, y_recv, own_sem, tp_send, tp_recv, down_send, down_rsem,
):
    own = (w0, w1, w2, w3, w4, w5, w6)
    full = (f0, f1, f2, f3, f4, f5, f6)
    f, g, t = lax.axis_index("fs"), lax.axis_index("grp"), lax.axis_index("tp")
    rows, columns = tok_ref.shape
    width = columns * n_tp
    seqs = rows // length
    bases = [sum(chunk_counts[:w]) for w in range(7)]

    def y_peer(k):
        return lax.rem(g + k, parts)

    def tp_peer(k):
        return lax.rem(t + k, n_tp)

    def span(w, half, c):
        size = own[w].shape[0] // parts
        piece = size // chunk_counts[w]
        start = half * size + c * piece
        return pl.ds(pl.multiple_of(start, 8), piece)

    def region(w, blk, half, c):
        return full[w].at[blk, span(w, half, c), :]

    barrier = pltpu.get_barrier_semaphore()
    for k in range(1, n_tp):
        pl.semaphore_signal(barrier, inc=1, device_id={"tp": tp_peer(k)}, device_id_type=MESH)
    for k in range(1, parts):
        pl.semaphore_signal(barrier, inc=1, device_id={"grp": y_peer(k)}, device_id_type=MESH)

    @pl.when(f < n - 1)
    def _():
        pl.semaphore_signal(barrier, inc=1, device_id={"fs": f + 1}, device_id_type=MESH)

    @pl.when(f > 0)
    def _():
        pl.semaphore_signal(barrier, inc=1, device_id={"fs": f - 1}, device_id_type=MESH)

    neighbours = lax.min(f, 1) + lax.min(n - 1 - f, 1)
    pl.semaphore_wait(barrier, n_tp - 1 + parts - 1 + neighbours)

    def z_copy(w, c, blk, src, step):
        send = right_send if step > 0 else left_send
        return pltpu.make_async_remote_copy(
            src_ref=src, dst_ref=region(w, blk, g, c),
            send_sem=send.at[bases[w] + c, blk], recv_sem=z_recv.at[bases[w] + c, blk],
            device_id={"fs": f + step}, device_id_type=MESH,
        )

    def y_copy(w, c, blk, half, k, peer):
        return pltpu.make_async_remote_copy(
            src_ref=region(w, blk, half, c), dst_ref=region(w, blk, half, c),
            send_sem=y_send.at[bases[w] + c, blk, k - 1], recv_sem=y_recv.at[bases[w] + c, blk, k - 1],
            device_id={"grp": peer}, device_id_type=MESH,
        )

    def start_own(w):
        @pl.loop(0, chunk_counts[w])
        def _(c):
            src = own[w].at[span(w, g, c), :]

            @pl.when(f < n - 1)
            def _():
                z_copy(w, c, f, src, 1).start()

            @pl.when(f > 0)
            def _():
                z_copy(w, c, f, src, -1).start()

    def receive(w, s):
        left, right = f - 1 - s, f + 1 + s

        @pl.loop(0, chunk_counts[w])
        def _(c):
            def arrived(blk, step):
                z_copy(w, c, blk, region(w, blk, g, c), -step).wait_recv()
                onward = (f < n - 1) if step > 0 else (f > 0)

                @pl.when(onward)
                def _():
                    z_copy(w, c, blk, region(w, blk, g, c), step).start()

                for k in range(1, parts):
                    y_copy(w, c, blk, g, k, y_peer(k)).start()

            @pl.when(left >= 0)
            def _():
                arrived(left, 1)

            @pl.when(right < n)
            def _():
                arrived(right, -1)

    def finish(w, s):
        @pl.loop(0, chunk_counts[w])
        def _(c):
            for k in range(1, parts):
                source = lax.rem(g + parts - k, parts)
                for blk, there in ((f - 1 - s, f - 1 - s >= 0), (f + 1 + s, f + 1 + s < n)):
                    @pl.when(there)
                    def _():
                        y_copy(w, c, blk, source, k, source).wait_recv()

    def own_copy(w):
        return pltpu.make_async_copy(own[w], full[w].at[f], own_sem.at[w])

    def tp_copy(stage, k, src, dst, peer):
        return pltpu.make_async_remote_copy(
            src_ref=src, dst_ref=dst, send_sem=tp_send.at[stage, k - 1], recv_sem=tp_recv.at[stage, k - 1],
            device_id={"tp": peer}, device_id_type=MESH,
        )

    def own_columns(owner):
        return pl.ds(pl.multiple_of(owner * columns, 128), columns)

    def source_of(k):
        return lax.rem(t + n_tp - k, n_tp)

    for w in range(MIXER):
        start_own(w)
    for k in range(1, n_tp):
        tp_copy(0, k, tok_ref, tok_full.at[:, own_columns(t)], tp_peer(k)).start()
    for w in range(7):
        own_copy(w).start()
    own_tokens = pltpu.make_async_copy(tok_ref, tok_full.at[:, own_columns(t)], own_sem.at[7])
    own_tokens.start()
    for w in range(MIXER):
        for s in range(n - 1):
            receive(w, s)
        if w == 2:
            start_own(GATE)

    def norm_rows(source, gain):
        size = 32

        @pl.loop(0, rows // size)
        def _(i):
            at = pl.ds(pl.multiple_of(i * size, size), size)
            values = source[at, :].astype(F32)
            scale = lax.rsqrt(jnp.sum(values * values, axis=1, keepdims=True) / width + 1e-06)
            normed[at, :] = (values * scale * gain[...]).astype(BF16)

    own_tokens.wait()
    for k in range(1, n_tp):
        tp_copy(0, k, tok_ref, tok_full.at[:, own_columns(source_of(k))], tp_peer(k)).wait_recv()
    norm_rows(tok_full, mix_gain)
    channels = w0.shape[1]
    for w in range(MIXER):
        own_copy(w).wait()
        for s in range(n - 1):
            finish(w, s)
    for w in range(3):
        weight = full[w][...].reshape(width, channels)
        proj[w] = jnp.dot(normed[...], weight, preferred_element_type=F32).astype(BF16)
    taps = taps_ref[:, pl.ds(pl.multiple_of(t * channels, 128), channels)]
    tap_count = taps_ref.shape[0]

    @pl.loop(0, seqs)
    def _(i):
        at = pl.ds(pl.multiple_of(i * length, length), length)
        product = proj[1, at, :].astype(F32) * proj[2, at, :].astype(F32)
        position = lax.broadcasted_iota(jnp.int32, product.shape, 0)
        conv = jnp.zeros_like(product)
        for offset in range(tap_count):
            shift = tap_count - 1 - offset
            moved = product if shift == 0 else jnp.where(position >= shift, pltpu.roll(product, shift, 0), 0.0)
            conv = conv + taps[offset : offset + 1, :] * moved
        gated[at, :] = (proj[0, at, :].astype(F32) * conv).astype(BF16)

    block = w3.shape[1]

    @pl.loop(0, n)
    def _(b):
        at = pl.ds(pl.multiple_of(b * block, 128), block)
        mix_part[:, at] = jnp.dot(gated[...], full[3][b], preferred_element_type=F32).astype(BF16)

    for k in range(1, n_tp):
        peer = tp_peer(k)
        tp_copy(1, k, mix_part.at[:, own_columns(peer)], mix_recv.at[k - 1], peer).start()

    for s in range(n - 1):
        if s == n - 2:
            start_own(UP)
        receive(GATE, s)

    for k in range(1, n_tp):
        tp_copy(1, k, mix_part.at[:, own_columns(t)], mix_recv.at[k - 1], source_of(k)).wait_recv()

    @pl.loop(0, rows // 64)
    def _(i):
        at = pl.ds(pl.multiple_of(i * 64, 64), 64)
        total = mix_part[at, own_columns(t)].astype(F32)
        for k in range(1, n_tp):
            total = total + mix_recv[k - 1, at, :].astype(F32)
        first_full[at, own_columns(t)] = (tok_ref[at, :].astype(F32) + total).astype(BF16)

    for k in range(1, n_tp):
        mine = first_full.at[:, own_columns(t)]
        tp_copy(2, k, mine, mine, tp_peer(k)).start()

    for s in range(n - 1):
        if s == n - 2:
            start_own(DOWN)
        receive(UP, s)

    for k in range(1, n_tp):
        theirs = first_full.at[:, own_columns(source_of(k))]
        tp_copy(2, k, theirs, theirs, source_of(k)).wait_recv()
    norm_rows(first_full, ffn_gain)
    for w in (GATE, UP):
        own_copy(w).wait()
        for s in range(n - 1):
            finish(w, s)

    units = w4.shape[1]

    def hidden_tile(start, size):
        at = pl.ds(start, size)
        gate = jnp.dot(normed[...], full[GATE][:, :, at].reshape(width, size), preferred_element_type=F32)
        upward = jnp.dot(normed[...], full[UP][:, :, at].reshape(width, size), preferred_element_type=F32)
        hidden[:, at] = (gate / (1.0 + jnp.exp(-gate)) * upward).astype(BF16)

    @pl.loop(0, units // 256)
    def _(j):
        hidden_tile(pl.multiple_of(j * 256, 256), 256)

    if units % 256:
        hidden_tile(units // 256 * 256, units % 256)

    wide = w6.shape[1]
    piece = min(wide, columns)
    per_block, per_owner = wide // piece, columns // piece

    def down_copy(sender, owner, slot, start):
        k = lax.rem(owner - sender + n_tp, n_tp)
        inside = pl.ds(pl.multiple_of(slot * piece, 128), piece)
        return pltpu.make_async_remote_copy(
            src_ref=down_part.at[:, pl.ds(start, piece)], dst_ref=down_recv.at[k, :, inside],
            send_sem=down_send.at[k, slot], recv_sem=down_rsem.at[k, slot],
            device_id={"tp": owner}, device_id_type=MESH,
        )

    def down_block(b):
        for p in range(per_block):
            start = pl.multiple_of(b * wide + p * piece, 128)
            owner = (b * wide + p * piece) // columns
            slot = lax.rem(b * per_block + p, per_owner)
            weight = full[DOWN][b][:, p * piece : (p + 1) * piece]
            down_part[:, pl.ds(start, piece)] = jnp.dot(
                hidden[...], weight, preferred_element_type=F32
            ).astype(BF16)

            @pl.when(owner != t)
            def _():
                down_copy(t, owner, slot, start).start()

    own_copy(DOWN).wait()
    down_block(f)

    @pl.loop(0, n - 1)
    def _(s):
        receive(DOWN, s)
        finish(DOWN, s)

        @pl.loop(0, 2)
        def _(side):
            b = lax.select(side == 0, f - 1 - s, f + 1 + s)

            @pl.when((b >= 0) & (b < n))
            def _():
                down_block(b)

    for k in range(1, n_tp):
        for slot in range(per_owner):
            down_copy(source_of(k), t, slot, 0).wait_recv()

    def second_rows(i):
        at = pl.ds(pl.multiple_of(i * length, length), length)
        total = down_part[at, own_columns(t)].astype(F32)
        for k in range(1, n_tp):
            total = total + down_recv[k, at, :].astype(F32)
        return at, first_full[at, own_columns(t)].astype(F32) + total

    @pl.loop(0, seqs)
    def _(i):
        _, second = second_rows(i)
        squares = jnp.sum(second * second, axis=1, keepdims=True)
        wide_squares = jnp.transpose(jnp.broadcast_to(squares, (length, length)))
        sq_send[i] = wide_squares[:8, :]

    for k in range(1, n_tp):
        tp_copy(3, k, sq_send, sq_recv.at[k - 1], tp_peer(k)).start()
    for k in range(1, n_tp):
        tp_copy(3, k, sq_send, sq_recv.at[k - 1], source_of(k)).wait_recv()

    gain = out_gain[:, own_columns(t)]

    @pl.loop(0, seqs)
    def _(i):
        at, second = second_rows(i)
        squares = sq_send[i]
        for k in range(1, n_tp):
            squares = squares + sq_recv[k - 1, i]
        factor = column(lax.rsqrt(squares[:1, :] / width + 1e-06))
        out_ref[at, :] = (second * factor * gain).astype(BF16)

    for k in range(1, n_tp):
        tp_copy(0, k, tok_ref, tok_full.at[:, own_columns(t)], tp_peer(k)).wait_send()
        tp_copy(1, k, mix_part.at[:, own_columns(t)], mix_recv.at[k - 1], tp_peer(k)).wait_send()
        tp_copy(2, k, first_full.at[:, own_columns(t)], first_full.at[:, own_columns(t)], tp_peer(k)).wait_send()
        tp_copy(3, k, sq_send, sq_recv.at[k - 1], tp_peer(k)).wait_send()
        for slot in range(per_owner):
            down_copy(t, tp_peer(k), slot, 0).wait_send()
    for w in range(7):
        @pl.loop(0, chunk_counts[w])
        def _(c):
            @pl.loop(0, n)
            def _(blk):
                here = region(w, blk, g, c)

                @pl.when((f < n - 1) & (blk <= f))
                def _():
                    z_copy(w, c, blk, here, 1).wait_send()

                @pl.when((f > 0) & (blk >= f))
                def _():
                    z_copy(w, c, blk, here, -1).wait_send()

                @pl.when(blk != f)
                def _():
                    for k in range(1, parts):
                        y_copy(w, c, blk, g, k, y_peer(k)).wait_send()


def solution(mesh):
    n, parts, n_tp = mesh.shape["fs"], mesh.shape["grp"], mesh.shape["tp"]

    def local(tokens, mix_gain, outer, inner, value, taps, mix_out, ffn_gain, gate, up, down, out_gain):
        seqs, length, columns = tokens.shape
        rows, width = seqs * length, columns * n_tp
        weights = (outer, inner, value, mix_out, gate, up, down)
        counts = tuple(1 if w < MIXER else chunks_of(a.shape[0] // parts) for w, a in enumerate(weights))
        slots = sum(counts)
        channels, units = outer.shape[1], gate.shape[1]
        others, y_others = max(n_tp - 1, 1), max(parts - 1, 1)
        per_owner = columns // min(down.shape[1], columns)
        dma = pltpu.SemaphoreType.DMA
        scratch = [pltpu.VMEM((n,) + a.shape, BF16) for a in weights]
        scratch += [
            pltpu.VMEM((rows, width), BF16),
            pltpu.VMEM((rows, width), BF16),
            pltpu.VMEM((3, rows, channels), BF16),
            pltpu.VMEM((rows, channels), BF16),
            pltpu.VMEM((rows, width), BF16),
            pltpu.VMEM((others, rows, columns), BF16),
            pltpu.VMEM((rows, width), BF16),
            pltpu.VMEM((rows, units), BF16),
            pltpu.VMEM((rows, width), BF16),
            pltpu.VMEM((n_tp, rows, columns), BF16),
            pltpu.VMEM((seqs, 8, length), F32),
            pltpu.VMEM((others, seqs, 8, length), F32),
            dma((slots, n)), dma((slots, n)), dma((slots, n)),
            dma((slots, n, y_others)), dma((slots, n, y_others)),
            dma((8,)), dma((4, others)), dma((4, others)),
            dma((n_tp, per_owner)), dma((n_tp, per_owner)),
        ]
        out = pl.pallas_call(
            functools.partial(kernel, n, parts, n_tp, length, counts),
            out_shape=jax.ShapeDtypeStruct((rows, columns), BF16),
            in_specs=[pl.BlockSpec(memory_space=pltpu.VMEM)] * 12,
            out_specs=pl.BlockSpec(memory_space=pltpu.VMEM),
            scratch_shapes=scratch,
            compiler_params=pltpu.CompilerParams(
                collective_id=0, has_side_effects=True, vmem_limit_bytes=60 * 1024 * 1024
            ),
        )(
            tokens.reshape(rows, columns), mix_gain[None], outer, inner, value, taps, mix_out,
            ffn_gain[None], gate, up, down, out_gain[None],
        )
        return out.reshape(seqs, length, columns)

    in_specs = (
        P(("grp", "fs"), None, "tp"), P(), P("fs", "tp"), P("fs", "tp"), P("fs", "tp"), P(), P("tp", "fs"),
        P(), P("fs", "tp"), P("fs", "tp"), P("tp", "fs"), P(),
    )
    out_specs = P(("grp", "fs"), None, "tp")
    return jax.shard_map(local, mesh=mesh, in_specs=in_specs, out_specs=out_specs, check_vma=False)
```

```python
import functools

import jax
import jax.numpy as jnp
from jax import lax
from jax.experimental import pallas as pl
from jax.experimental.pallas import tpu as pltpu
from jax.sharding import PartitionSpec as P

MESH = pl.DeviceIdType.MESH
F32 = jnp.float32
BF16 = jnp.bfloat16
MIXER = 4
GATE, UP, DOWN = 4, 5, 6


def chunks_of(half):
    return next(count for count in (4, 2, 1) if half % (count * 16) == 0 or count == 1)


def column(rows):
    wide = jnp.broadcast_to(rows, (rows.shape[1], rows.shape[1]))
    return jnp.transpose(wide)[:, :1]


def kernel(
    n, parts, n_tp, length, chunk_counts,
    tok_ref, mix_gain, w0, w1, w2, taps_ref, w3, ffn_gain, w4, w5, w6, out_gain,
    out_ref,
    f0, f1, f2, f3, f4, f5, f6,
    tok_full, normed, proj, gated, part, pair_recv, far_recv, first_full, hidden, returned, sq_send, sq_recv,
    right_send, left_send, z_recv, y_send, y_recv, own_sem, pair_ss, pair_rs, far_ss, far_rs,
    down_pair_ss, down_pair_rs, down_far_ss, down_far_rs, sq_ss, sq_rs, guest_sem,
):
    own = (w0, w1, w2, w3, w4, w5, w6)
    full = (f0, f1, f2, f3, f4, f5, f6)
    f, g, t = lax.axis_index("fs"), lax.axis_index("grp"), lax.axis_index("tp")
    rows, columns = tok_ref.shape
    width = columns * n_tp
    seqs = rows // length
    bases = [sum(chunk_counts[:w]) for w in range(7)]

    def y_peer(k):
        return lax.rem(g + k, parts)

    def tp_peer(k):
        return lax.rem(t + k, n_tp)

    def span(w, half, c):
        size = own[w].shape[0] // parts
        piece = size // chunk_counts[w]
        start = half * size + c * piece
        return pl.ds(pl.multiple_of(start, 8), piece)

    def region(w, blk, half, c):
        return full[w].at[blk, span(w, half, c), :]

    barrier = pltpu.get_barrier_semaphore()
    for k in range(1, n_tp):
        pl.semaphore_signal(barrier, inc=1, device_id={"tp": tp_peer(k)}, device_id_type=MESH)
    for k in range(1, parts):
        pl.semaphore_signal(barrier, inc=1, device_id={"grp": y_peer(k)}, device_id_type=MESH)

    @pl.when(f < n - 1)
    def _():
        pl.semaphore_signal(barrier, inc=1, device_id={"fs": f + 1}, device_id_type=MESH)

    @pl.when(f > 0)
    def _():
        pl.semaphore_signal(barrier, inc=1, device_id={"fs": f - 1}, device_id_type=MESH)

    neighbours = lax.min(f, 1) + lax.min(n - 1 - f, 1)
    pl.semaphore_wait(barrier, n_tp - 1 + parts - 1 + neighbours)

    def z_copy(w, c, blk, src, step):
        send = right_send if step > 0 else left_send
        return pltpu.make_async_remote_copy(
            src_ref=src, dst_ref=region(w, blk, g, c),
            send_sem=send.at[bases[w] + c, blk], recv_sem=z_recv.at[bases[w] + c, blk],
            device_id={"fs": f + step}, device_id_type=MESH,
        )

    def y_copy(w, c, blk, half, k, peer):
        return pltpu.make_async_remote_copy(
            src_ref=region(w, blk, half, c), dst_ref=region(w, blk, half, c),
            send_sem=y_send.at[bases[w] + c, blk, k - 1], recv_sem=y_recv.at[bases[w] + c, blk, k - 1],
            device_id={"grp": peer}, device_id_type=MESH,
        )

    first_host, last_host = 1, n - 2
    is_host = (f >= first_host) & (f <= last_host)

    def start_own(w):
        @pl.loop(0, chunk_counts[w])
        def _(c):
            src = own[w].at[span(w, g, c), :]

            @pl.when(f + 1 <= last_host)
            def _():
                z_copy(w, c, f, src, 1).start()

            @pl.when(f - 1 >= first_host)
            def _():
                z_copy(w, c, f, src, -1).start()

    def other_half(w, c, k):
        half = lax.rem(g + parts - k, parts)
        inward = lax.select(f == 0, 1, n - 2)
        return pltpu.make_async_remote_copy(
            src_ref=own[w].at[span(w, half, c), :], dst_ref=region(w, f, half, c),
            send_sem=y_send.at[bases[w] + c, f, k - 1], recv_sem=y_recv.at[bases[w] + c, f, k - 1],
            device_id={"fs": inward}, device_id_type=MESH,
        )

    def receive(w, s):
        left, right = f - 1 - s, f + 1 + s

        @pl.loop(0, chunk_counts[w])
        def _(c):
            def arrived(blk, step, whole):
                z_copy(w, c, blk, region(w, blk, g, c), -step).wait_recv()
                onward = (f + 1 <= last_host) if step > 0 else (f - 1 >= first_host)

                @pl.when(onward)
                def _():
                    z_copy(w, c, blk, region(w, blk, g, c), step).start()

                def share():
                    for k in range(1, parts):
                        y_copy(w, c, blk, g, k, y_peer(k)).start()

                if s == 0:
                    pl.when(jnp.logical_not(whole))(share)
                else:
                    share()

            @pl.when(right < n)
            def _():
                arrived(right, -1, right == n - 1)

            @pl.when(left >= 0)
            def _():
                arrived(left, 1, left == 0)

    def finish(w, s):
        @pl.loop(0, chunk_counts[w])
        def _(c):
            for k in range(1, parts):
                source = lax.rem(g + parts - k, parts)
                for blk, there in ((f - 1 - s, f - 1 - s >= 0), (f + 1 + s, f + 1 + s < n)):
                    @pl.when(there)
                    def _():
                        y_copy(w, c, blk, source, k, source).wait_recv()

    def own_copy(w):
        return pltpu.make_async_copy(own[w], full[w].at[f], own_sem.at[w])

    def own_columns(owner):
        return pl.ds(pl.multiple_of(owner * columns, 128), columns)

    chips = n_tp // 2
    core = lax.rem(t, 2)
    pair = t + 1 - 2 * core

    def ahead(k, start=None):
        return lax.rem((t if start is None else start) + 2 * k, n_tp)

    def behind(k, start=None):
        return lax.rem((t if start is None else start) + n_tp - 2 * k, n_tp)

    def set_rows(r):
        return pl.ds(r * rows, rows)

    def pair_copy(stage, r, k, src, dst):
        return pltpu.make_async_remote_copy(
            src_ref=src, dst_ref=dst, send_sem=pair_ss.at[stage, r, k], recv_sem=pair_rs.at[stage, r, k],
            device_id={"tp": pair}, device_id_type=MESH,
        )

    def far_copy(stage, r, k, src, dst, peer):
        return pltpu.make_async_remote_copy(
            src_ref=src, dst_ref=dst, send_sem=far_ss.at[stage, r, k], recv_sem=far_rs.at[stage, r, k],
            device_id={"tp": peer}, device_id_type=MESH,
        )

    def block_of(buf, r, owner):
        return buf.at[set_rows(r), own_columns(owner)]

    def gather_send(buf, stage, r):
        mine = block_of(buf, r, t)
        for k in range(1, chips):
            far_copy(stage, r, k, mine, mine, ahead(k)).start()
        pair_copy(stage, r, 0, mine, mine).start()

    def gather_relay(buf, stage, r):
        for k in range(1, chips):
            theirs = block_of(buf, r, behind(k))
            far_copy(stage, r, k, theirs, theirs, behind(k)).wait_recv()
            pair_copy(stage, r, k, theirs, theirs).start()

    def gather_finish(buf, stage, r):
        for k in range(chips):
            theirs = block_of(buf, r, behind(k, pair))
            pair_copy(stage, r, k, theirs, theirs).wait_recv()

    def gather_sent(buf, stage, r):
        mine = block_of(buf, r, t)
        for k in range(1, chips):
            far_copy(stage, r, k, mine, mine, ahead(k)).wait_send()
        for k in range(chips):
            pair_copy(stage, r, k, mine, mine).wait_send()

    def to_pair(r, k):
        return pair_copy(1, r, k, block_of(part, r, ahead(k, pair)), pair_recv.at[r, k])

    def to_far(r, k):
        return far_copy(1, r, k, block_of(part, r, ahead(k)), far_recv.at[r, k], ahead(k))

    def sum_send(r):
        for k in range(chips - 1, -1, -1):
            to_pair(r, k).start()

    def sum_relay(r):
        for k in range(1, chips):
            to_pair(r, k).wait_recv()

            @pl.loop(0, rows // 64)
            def _(i):
                inside = pl.ds(pl.multiple_of(i * 64, 64), 64)
                at = pl.ds(pl.multiple_of(r * rows + i * 64, 64), 64)
                both = part[at, own_columns(ahead(k))].astype(F32) + pair_recv[r, k, inside, :].astype(F32)
                part[at, own_columns(ahead(k))] = both.astype(BF16)

            to_far(r, k).start()

    def summed(r, start, size):
        inside = pl.ds(pl.multiple_of(start, size), size)
        at = pl.ds(pl.multiple_of(r * rows + start, size), size)
        total = part[at, own_columns(t)].astype(F32) + pair_recv[r, 0, inside, :].astype(F32)
        for k in range(1, chips):
            total = total + far_recv[r, k, inside, :].astype(F32)
        return at, total

    def first_rows(r):
        to_pair(r, 0).wait_recv()
        for k in range(1, chips):
            to_far(r, k).wait_recv()

        @pl.loop(0, rows // 64)
        def _(i):
            at, total = summed(r, i * 64, 64)
            first_full[at, own_columns(t)] = (tok_full[at, own_columns(t)].astype(F32) + total).astype(BF16)

    def norm_rows(source, gain, r):
        size = 32

        @pl.loop(0, rows // size)
        def _(i):
            at = pl.ds(pl.multiple_of(r * rows + i * size, size), size)
            values = source[at, :].astype(F32)
            scale = lax.rsqrt(jnp.sum(values * values, axis=1, keepdims=True) / width + 1e-06)
            normed[at, :] = (values * scale * gain[...]).astype(BF16)

    channels = w0.shape[1]
    block = w3.shape[1]
    units = w4.shape[1]
    tap_count = taps_ref.shape[0]

    def mixer(r):
        for w in range(3):
            weight = full[w][...].reshape(width, channels)
            proj[w] = jnp.dot(normed[set_rows(r), :], weight, preferred_element_type=F32).astype(BF16)
        taps = taps_ref[:, pl.ds(pl.multiple_of(t * channels, 128), channels)]

        @pl.loop(0, seqs)
        def _(i):
            at = pl.ds(pl.multiple_of(i * length, length), length)
            product = proj[1, at, :].astype(F32) * proj[2, at, :].astype(F32)
            position = lax.broadcasted_iota(jnp.int32, product.shape, 0)
            conv = jnp.zeros_like(product)
            for offset in range(tap_count):
                shift = tap_count - 1 - offset
                moved = product if shift == 0 else jnp.where(position >= shift, pltpu.roll(product, shift, 0), 0.0)
                conv = conv + taps[offset : offset + 1, :] * moved
            gated[at, :] = (proj[0, at, :].astype(F32) * conv).astype(BF16)

        @pl.loop(0, n)
        def _(b):
            at = pl.ds(pl.multiple_of(b * block, 128), block)
            part[set_rows(r), at] = jnp.dot(gated[...], full[3][b], preferred_element_type=F32).astype(BF16)

    def hidden_tile(r, start, size):
        at = pl.ds(start, size)
        left = normed[set_rows(r), :]
        gate = jnp.dot(left, full[GATE][:, :, at].reshape(width, size), preferred_element_type=F32)
        upward = jnp.dot(left, full[UP][:, :, at].reshape(width, size), preferred_element_type=F32)
        hidden[set_rows(r), at] = (gate / (1.0 + jnp.exp(-gate)) * upward).astype(BF16)

    def hidden_rows(r):
        @pl.loop(0, units // 256)
        def _(j):
            hidden_tile(r, pl.multiple_of(j * 256, 256), 256)

        if units % 256:
            hidden_tile(r, units // 256 * 256, units % 256)

    wide = w6.shape[1]
    piece = min(wide, columns)
    per_block, per_owner = wide // piece, columns // piece

    def down_to_pair(r, k, slot, start):
        inside = pl.ds(pl.multiple_of(slot * piece, 128), piece)
        return pltpu.make_async_remote_copy(
            src_ref=part.at[set_rows(r), pl.ds(start, piece)], dst_ref=pair_recv.at[r, k, :, inside],
            send_sem=down_pair_ss.at[r, k, slot], recv_sem=down_pair_rs.at[r, k, slot],
            device_id={"tp": pair}, device_id_type=MESH,
        )

    def down_to_far(r, k, slot, start):
        inside = pl.ds(pl.multiple_of(slot * piece, 128), piece)
        return pltpu.make_async_remote_copy(
            src_ref=part.at[set_rows(r), pl.ds(start, piece)], dst_ref=far_recv.at[r, k, :, inside],
            send_sem=down_far_ss.at[r, k, slot], recv_sem=down_far_rs.at[r, k, slot],
            device_id={"tp": lax.rem(t + 2 * k, n_tp)}, device_id_type=MESH,
        )

    def down_block(b):
        for p in range(per_block):
            start = pl.multiple_of(b * wide + p * piece, 128)
            owner = (b * wide + p * piece) // columns
            slot = lax.rem(b * per_block + p, per_owner)
            k = lax.rem(owner // 2 - t // 2 + chips, chips)
            lane = lax.rem(owner, 2) == core

            @pl.loop(0, 2)
            def _(turn):
                r = 1 - turn
                at = pl.ds(pl.multiple_of(r * rows, rows), rows)
                weight = full[DOWN][b][:, p * piece : (p + 1) * piece]
                part[at, pl.ds(start, piece)] = jnp.dot(
                    hidden[at, :], weight, preferred_element_type=F32
                ).astype(BF16)

                @pl.when(jnp.logical_not(lane))
                def _():
                    down_to_pair(r, k, slot, start).start()

            @pl.when(lane & (k > 0))
            def _():
                for r in (1, 0):
                    down_to_pair(r, k, slot, start).wait_recv()
                    inside = pl.ds(pl.multiple_of(slot * piece, 128), piece)

                    @pl.loop(0, rows // 64)
                    def _(i):
                        here = pl.ds(pl.multiple_of(i * 64, 64), 64)
                        at = pl.ds(pl.multiple_of(r * rows + i * 64, 64), 64)
                        both = part[at, pl.ds(start, piece)].astype(F32) + pair_recv[r, k, here, inside].astype(F32)
                        part[at, pl.ds(start, piece)] = both.astype(BF16)

                    down_to_far(r, k, slot, start).start()

    def square_copy(r, k, peer):
        return pltpu.make_async_remote_copy(
            src_ref=sq_send.at[r], dst_ref=sq_recv.at[r, k - 1], send_sem=sq_ss.at[r, k - 1],
            recv_sem=sq_rs.at[r, k - 1], device_id={"tp": peer}, device_id_type=MESH,
        )

    def squares_send(r):
        for slot in range(per_owner):
            down_to_pair(r, 0, slot, 0).wait_recv()
            for k in range(1, chips):
                down_to_far(r, k, slot, 0).wait_recv()

        @pl.loop(0, seqs)
        def _(i):
            at, total = summed(r, i * length, length)
            second = first_full[at, own_columns(t)].astype(F32) + total
            squares = jnp.sum(second * second, axis=1, keepdims=True)
            sq_send[r, i] = jnp.transpose(jnp.broadcast_to(squares, (length, length)))[:8, :]

        for k in range(1, n_tp):
            square_copy(r, k, lax.rem(t + k, n_tp)).start()

    def close(r, dst):
        for k in range(1, n_tp):
            square_copy(r, k, lax.rem(t + n_tp - k, n_tp)).wait_recv()
        gain = out_gain[:, own_columns(t)]

        @pl.loop(0, seqs)
        def _(i):
            at, total = summed(r, i * length, length)
            second = first_full[at, own_columns(t)].astype(F32) + total
            squares = sq_send[r, i]
            for k in range(1, n_tp):
                squares = squares + sq_recv[r, k - 1, i]
            factor = column(lax.rsqrt(squares[:1, :] / width + 1e-06))
            inside = pl.ds(pl.multiple_of(i * length, length), length)
            dst[inside, :] = (second * factor * gain).astype(BF16)

    guest = lax.select(f == 1, 0, n - 1)
    has_guest = (f == 1) | (f == n - 2)
    inner = lax.select(f == 0, 1, n - 2)

    def tokens_in(device):
        return pltpu.make_async_remote_copy(
            src_ref=tok_ref, dst_ref=block_of(tok_full, 1, t), send_sem=guest_sem.at[0], recv_sem=guest_sem.at[1],
            device_id={"fs": device}, device_id_type=MESH,
        )

    def result_out(device):
        return pltpu.make_async_remote_copy(
            src_ref=returned, dst_ref=returned, send_sem=guest_sem.at[2], recv_sem=guest_sem.at[3],
            device_id={"fs": device}, device_id_type=MESH,
        )

    @pl.when(jnp.logical_not(is_host))
    def _():
        def halves(w, wait):
            @pl.loop(0, chunk_counts[w])
            def _(c):
                for k in range(1, parts):
                    if wait:
                        other_half(w, c, k).wait_send()
                    else:
                        other_half(w, c, k).start()

        tokens_in(inner).start()
        for w in range(MIXER):
            start_own(w)
        for w in range(MIXER):
            halves(w, False)
        for w in range(MIXER, 7):
            start_own(w)
            halves(w, False)
        tokens_in(inner).wait_send()
        for w in range(7):
            halves(w, True)

            @pl.loop(0, chunk_counts[w])
            def _(c):
                src = own[w].at[span(w, g, c), :]

                @pl.when(f == 0)
                def _():
                    z_copy(w, c, f, src, 1).wait_send()

                @pl.when(f == n - 1)
                def _():
                    z_copy(w, c, f, src, -1).wait_send()

        result_out(inner).wait_recv()
        out_ref[...] = returned[...]

    @pl.when(is_host)
    def _():
        own_tokens = pltpu.make_async_copy(tok_ref, block_of(tok_full, 0, t), own_sem.at[7])
        own_tokens.start()
        for w in range(MIXER):
            start_own(w)
        for w in range(7):
            own_copy(w).start()
        own_tokens.wait()
        gather_send(tok_full, 0, 0)
        steps = range(n - 2)
        for s in steps:
            receive(0, s)

        @pl.when(has_guest)
        def _():
            tokens_in(guest).wait_recv()

        gather_send(tok_full, 0, 1)
        gather_relay(tok_full, 0, 0)
        for w in range(1, MIXER):
            for s in steps:
                receive(w, s)
        start_own(GATE)
        gather_finish(tok_full, 0, 0)
        norm_rows(tok_full, mix_gain, 0)
        for w in range(MIXER):
            own_copy(w).wait()
            for s in steps:
                finish(w, s)
        mixer(0)
        sum_send(0)
        gather_relay(tok_full, 0, 1)
        receive(GATE, 0)
        start_own(UP)
        gather_finish(tok_full, 0, 1)
        norm_rows(tok_full, mix_gain, 1)
        sum_relay(0)
        mixer(1)
        sum_send(1)
        first_rows(0)
        gather_send(first_full, 2, 0)
        sum_relay(1)
        for s in steps[1:]:
            receive(GATE, s)
        receive(UP, 0)
        start_own(DOWN)
        gather_relay(first_full, 2, 0)
        first_rows(1)
        gather_send(first_full, 2, 1)
        gather_finish(first_full, 2, 0)
        norm_rows(first_full, ffn_gain, 0)
        for s in steps[1:]:
            receive(UP, s)
        gather_relay(first_full, 2, 1)
        for w in (GATE, UP):
            own_copy(w).wait()
            for s in steps:
                finish(w, s)
        hidden_rows(0)
        receive(DOWN, 0)
        gather_finish(first_full, 2, 1)
        norm_rows(first_full, ffn_gain, 1)
        hidden_rows(1)
        for r in range(2):
            for k in range(chips):
                to_pair(r, k).wait_send()
            for k in range(1, chips):
                to_far(r, k).wait_send()
        own_copy(DOWN).wait()
        down_block(f)

        for s in steps:
            if s > 0:
                receive(DOWN, s)
            finish(DOWN, s)

            @pl.loop(0, 2)
            def _(side):
                b = lax.select(side == 0, f - 1 - s, f + 1 + s)

                @pl.when((b >= 0) & (b < n))
                def _():
                    down_block(b)

        squares_send(1)
        squares_send(0)
        close(1, returned)

        @pl.when(has_guest)
        def _():
            result_out(guest).start()

        close(0, out_ref)

        @pl.when(has_guest)
        def _():
            result_out(guest).wait_send()

        for r in range(2):
            gather_sent(tok_full, 0, r)
            gather_sent(first_full, 2, r)
            for k in range(1, n_tp):
                square_copy(r, k, lax.rem(t + k, n_tp)).wait_send()
            for slot in range(per_owner):
                for k in range(chips):
                    down_to_pair(r, k, slot, 0).wait_send()
                for k in range(1, chips):
                    down_to_far(r, k, slot, 0).wait_send()
        for w in range(7):
            @pl.loop(0, chunk_counts[w])
            def _(c):
                @pl.loop(0, n)
                def _(blk):
                    here = region(w, blk, g, c)

                    @pl.when((f + 1 <= last_host) & (blk <= f))
                    def _():
                        z_copy(w, c, blk, here, 1).wait_send()

                    @pl.when((f - 1 >= first_host) & (blk >= f))
                    def _():
                        z_copy(w, c, blk, here, -1).wait_send()

                    whole = ((blk == 0) & (f == 1)) | ((blk == n - 1) & (f == n - 2))

                    @pl.when((blk != f) & jnp.logical_not(whole))
                    def _():
                        for k in range(1, parts):
                            y_copy(w, c, blk, g, k, y_peer(k)).wait_send()


def solution(mesh):
    n, parts, n_tp = mesh.shape["fs"], mesh.shape["grp"], mesh.shape["tp"]

    def local(tokens, mix_gain, outer, inner, value, taps, mix_out, ffn_gain, gate, up, down, out_gain):
        seqs, length, columns = tokens.shape
        rows, width = seqs * length, columns * n_tp
        weights = (outer, inner, value, mix_out, gate, up, down)
        counts = tuple(1 if w < MIXER else chunks_of(a.shape[0] // parts) for w, a in enumerate(weights))
        slots = sum(counts)
        channels, units = outer.shape[1], gate.shape[1]
        others, y_others = max(n_tp - 1, 1), max(parts - 1, 1)
        per_owner = columns // min(down.shape[1], columns)
        dma = pltpu.SemaphoreType.DMA
        scratch = [pltpu.VMEM((n,) + a.shape, BF16) for a in weights]
        chips = n_tp // 2
        scratch += [
            pltpu.VMEM((2 * rows, width), BF16),
            pltpu.VMEM((2 * rows, width), BF16),
            pltpu.VMEM((3, rows, channels), BF16),
            pltpu.VMEM((rows, channels), BF16),
            pltpu.VMEM((2 * rows, width), BF16),
            pltpu.VMEM((2, chips, rows, columns), BF16),
            pltpu.VMEM((2, chips, rows, columns), BF16),
            pltpu.VMEM((2 * rows, width), BF16),
            pltpu.VMEM((2 * rows, units), BF16),
            pltpu.VMEM((rows, columns), BF16),
            pltpu.VMEM((2, seqs, 8, length), F32),
            pltpu.VMEM((2, others, seqs, 8, length), F32),
            dma((slots, n)), dma((slots, n)), dma((slots, n)),
            dma((slots, n, y_others)), dma((slots, n, y_others)),
            dma((8,)), dma((3, 2, chips)), dma((3, 2, chips)), dma((3, 2, chips)), dma((3, 2, chips)),
            dma((2, chips, per_owner)), dma((2, chips, per_owner)),
            dma((2, chips, per_owner)), dma((2, chips, per_owner)),
            dma((2, others)), dma((2, others)), dma((4,)),
        ]
        out = pl.pallas_call(
            functools.partial(kernel, n, parts, n_tp, length, counts),
            out_shape=jax.ShapeDtypeStruct((rows, columns), BF16),
            in_specs=[pl.BlockSpec(memory_space=pltpu.VMEM)] * 12,
            out_specs=pl.BlockSpec(memory_space=pltpu.VMEM),
            scratch_shapes=scratch,
            compiler_params=pltpu.CompilerParams(
                collective_id=0, has_side_effects=True, vmem_limit_bytes=62 * 1024 * 1024
            ),
        )(
            tokens.reshape(rows, columns), mix_gain[None], outer, inner, value, taps, mix_out,
            ffn_gain[None], gate, up, down, out_gain[None],
        )
        return out.reshape(seqs, length, columns)

    in_specs = (
        P(("grp", "fs"), None, "tp"), P(), P("fs", "tp"), P("fs", "tp"), P("fs", "tp"), P(), P("tp", "fs"),
        P(), P("fs", "tp"), P("fs", "tp"), P("tp", "fs"), P(),
    )
    out_specs = P(("grp", "fs"), None, "tp")
    return jax.shard_map(local, mesh=mesh, in_specs=in_specs, out_specs=out_specs, check_vma=False)
```

```python
import functools

import jax
import jax.numpy as jnp
from jax import lax
from jax.experimental import pallas as pl
from jax.experimental.pallas import tpu as pltpu
from jax.sharding import PartitionSpec as P

MESH = pl.DeviceIdType.MESH
F32 = jnp.float32
BF16 = jnp.bfloat16
MIXER = 4
GATE, UP, DOWN = 4, 5, 6
SHARED = 2


def chunks_of(half):
    return next(count for count in (4, 2, 1) if half % (count * 16) == 0 or count == 1)


def column(rows):
    wide = jnp.broadcast_to(rows, (rows.shape[1], rows.shape[1]))
    return jnp.transpose(wide)[:, :1]


def kernel(
    n, parts, n_tp, length, chunk_counts,
    tok_ref, mix_gain, w0, w1, w2, taps_ref, w3, ffn_gain, w4, w5, w6, out_gain,
    out_ref,
    f0, f1, f2, f3, f4, f5, f6,
    tok_full, normed, proj, gated, part, pair_recv, far_recv, first_full, hidden, returned, sq_send, sq_recv,
    right_send, left_send, z_recv, y_send, y_recv, own_sem, pair_ss, pair_rs, far_ss, far_rs,
    down_pair_ss, down_pair_rs, down_far_ss, down_far_rs, sq_ss, sq_rs, guest_sem,
):
    own = (w0, w1, w2, w3, w4, w5, w6)
    full = (f0, f1, f2, f3, f4, f5, f6)
    f, g, t = lax.axis_index("fs"), lax.axis_index("grp"), lax.axis_index("tp")
    rows, columns = tok_ref.shape
    width = columns * n_tp
    seqs = rows // length
    bases = [sum(chunk_counts[:w]) for w in range(7)]

    def y_peer(k):
        return lax.rem(g + k, parts)

    def tp_peer(k):
        return lax.rem(t + k, n_tp)

    def span(w, half, c):
        size = own[w].shape[0] // parts
        piece = size // chunk_counts[w]
        start = half * size + c * piece
        return pl.ds(pl.multiple_of(start, 8), piece)

    def region(w, blk, half, c):
        if w == DOWN:
            return full[w].at[blk, half_rows(half), strip(c)]
        return full[w].at[blk, span(w, half, c), :]

    def half_rows(half):
        size = w6.shape[0] // parts
        return pl.ds(pl.multiple_of(half * size, 8), size)

    def strip(c):
        size = w6.shape[1] // chunk_counts[DOWN]
        return pl.ds(pl.multiple_of(c * size, 128), size)

    def own_region(w, half, c):
        if w == DOWN:
            return own[w].at[half_rows(half), strip(c)]
        return own[w].at[span(w, half, c), :]

    barrier = pltpu.get_barrier_semaphore()
    for k in range(1, n_tp):
        pl.semaphore_signal(barrier, inc=1, device_id={"tp": tp_peer(k)}, device_id_type=MESH)
    for k in range(1, parts):
        pl.semaphore_signal(barrier, inc=1, device_id={"grp": y_peer(k)}, device_id_type=MESH)

    @pl.when(f < n - 1)
    def _():
        pl.semaphore_signal(barrier, inc=1, device_id={"fs": f + 1}, device_id_type=MESH)

    @pl.when(f > 0)
    def _():
        pl.semaphore_signal(barrier, inc=1, device_id={"fs": f - 1}, device_id_type=MESH)

    neighbours = lax.min(f, 1) + lax.min(n - 1 - f, 1)
    pl.semaphore_wait(barrier, n_tp - 1 + parts - 1 + neighbours)

    def z_copy(w, c, blk, src, step):
        send = right_send if step > 0 else left_send
        return pltpu.make_async_remote_copy(
            src_ref=src, dst_ref=region(w, blk, g, c),
            send_sem=send.at[bases[w] + c, blk], recv_sem=z_recv.at[bases[w] + c, blk],
            device_id={"fs": f + step}, device_id_type=MESH,
        )

    def y_copy(w, c, blk, half, k, peer):
        return pltpu.make_async_remote_copy(
            src_ref=region(w, blk, half, c), dst_ref=region(w, blk, half, c),
            send_sem=y_send.at[bases[w] + c, blk, k - 1], recv_sem=y_recv.at[bases[w] + c, blk, k - 1],
            device_id={"grp": peer}, device_id_type=MESH,
        )

    first_host, last_host = 1, n - 2
    is_host = (f >= first_host) & (f <= last_host)

    def start_own(w):
        @pl.loop(0, chunk_counts[w])
        def _(c):
            start_chunk(w, c)

    def start_chunk(w, c):
        src = own_region(w, g, c)

        @pl.when(f + 1 <= last_host)
        def _():
            z_copy(w, c, f, src, 1).start()

        @pl.when(f - 1 >= first_host)
        def _():
            z_copy(w, c, f, src, -1).start()

    def other_half(w, c, k):
        half = lax.rem(g + parts - k, parts)
        inward = lax.select(f == 0, 1, n - 2)
        return pltpu.make_async_remote_copy(
            src_ref=own_region(w, half, c), dst_ref=region(w, f, half, c),
            send_sem=y_send.at[bases[w] + c, f, k - 1], recv_sem=y_recv.at[bases[w] + c, f, k - 1],
            device_id={"fs": inward}, device_id_type=MESH,
        )

    def receive(w, s):
        @pl.loop(0, chunk_counts[w])
        def _(c):
            receive_chunk(w, s, c)

    def receive_chunk(w, s, c):
        left, right = f - 1 - s, f + 1 + s
        if True:
            def arrived(blk, step, whole):
                z_copy(w, c, blk, region(w, blk, g, c), -step).wait_recv()
                onward = (f + 1 <= last_host) if step > 0 else (f - 1 >= first_host)

                @pl.when(onward)
                def _():
                    z_copy(w, c, blk, region(w, blk, g, c), step).start()

                def share():
                    for k in range(1, parts):
                        y_copy(w, c, blk, g, k, y_peer(k)).start()

                if s == 0 and w >= SHARED:
                    pl.when(jnp.logical_not(whole))(share)
                else:
                    share()

            @pl.when(right < n)
            def _():
                arrived(right, -1, right == n - 1)

            @pl.when(left >= 0)
            def _():
                arrived(left, 1, left == 0)

    def finish(w, s):
        @pl.loop(0, chunk_counts[w])
        def _(c):
            finish_chunk(w, s, c)

    def finish_chunk(w, s, c):
        if True:
            for k in range(1, parts):
                source = lax.rem(g + parts - k, parts)
                for blk, there in ((f - 1 - s, f - 1 - s >= 0), (f + 1 + s, f + 1 + s < n)):
                    @pl.when(there)
                    def _():
                        y_copy(w, c, blk, source, k, source).wait_recv()

    def own_copy(w):
        return pltpu.make_async_copy(own[w], full[w].at[f], own_sem.at[w])

    def own_columns(owner):
        return pl.ds(pl.multiple_of(owner * columns, 128), columns)

    chips = n_tp // 2
    core = lax.rem(t, 2)
    pair = t + 1 - 2 * core

    def ahead(k, start=None):
        return lax.rem((t if start is None else start) + 2 * k, n_tp)

    def behind(k, start=None):
        return lax.rem((t if start is None else start) + n_tp - 2 * k, n_tp)

    def set_rows(r):
        return pl.ds(r * rows, rows)

    def pair_copy(stage, r, k, src, dst):
        return pltpu.make_async_remote_copy(
            src_ref=src, dst_ref=dst, send_sem=pair_ss.at[stage, r, k], recv_sem=pair_rs.at[stage, r, k],
            device_id={"tp": pair}, device_id_type=MESH,
        )

    def far_copy(stage, r, k, src, dst, peer):
        return pltpu.make_async_remote_copy(
            src_ref=src, dst_ref=dst, send_sem=far_ss.at[stage, r, k], recv_sem=far_rs.at[stage, r, k],
            device_id={"tp": peer}, device_id_type=MESH,
        )

    def block_of(buf, r, owner):
        return buf.at[set_rows(r), own_columns(owner)]

    def gather_send(buf, stage, r):
        mine = block_of(buf, r, t)
        for k in range(1, chips):
            far_copy(stage, r, k, mine, mine, ahead(k)).start()
        pair_copy(stage, r, 0, mine, mine).start()

    def gather_relay(buf, stage, r):
        for k in range(1, chips):
            theirs = block_of(buf, r, behind(k))
            far_copy(stage, r, k, theirs, theirs, behind(k)).wait_recv()
            pair_copy(stage, r, k, theirs, theirs).start()

    def gather_finish(buf, stage, r):
        for k in range(chips):
            theirs = block_of(buf, r, behind(k, pair))
            pair_copy(stage, r, k, theirs, theirs).wait_recv()

    def gather_sent(buf, stage, r):
        mine = block_of(buf, r, t)
        for k in range(1, chips):
            far_copy(stage, r, k, mine, mine, ahead(k)).wait_send()
        for k in range(chips):
            pair_copy(stage, r, k, mine, mine).wait_send()

    def to_pair(r, k):
        return pair_copy(1, r, k, block_of(part, r, ahead(k, pair)), pair_recv.at[r, k])

    def to_far(r, k):
        return far_copy(1, r, k, block_of(part, r, ahead(k)), far_recv.at[r, k], ahead(k))

    def sum_send(r):
        for k in range(chips - 1, -1, -1):
            to_pair(r, k).start()

    def sum_relay(r):
        for k in range(1, chips):
            to_pair(r, k).wait_recv()

            @pl.loop(0, rows // 64)
            def _(i):
                inside = pl.ds(pl.multiple_of(i * 64, 64), 64)
                at = pl.ds(pl.multiple_of(r * rows + i * 64, 64), 64)
                both = part[at, own_columns(ahead(k))].astype(F32) + pair_recv[r, k, inside, :].astype(F32)
                part[at, own_columns(ahead(k))] = both.astype(BF16)

            to_far(r, k).start()

    def summed(r, start, size):
        inside = pl.ds(pl.multiple_of(start, size), size)
        at = pl.ds(pl.multiple_of(r * rows + start, size), size)
        total = part[at, own_columns(t)].astype(F32) + pair_recv[r, 0, inside, :].astype(F32)
        for k in range(1, chips):
            total = total + far_recv[r, k, inside, :].astype(F32)
        return at, total

    def first_rows(r):
        to_pair(r, 0).wait_recv()
        for k in range(1, chips):
            to_far(r, k).wait_recv()

        @pl.loop(0, rows // 64)
        def _(i):
            at, total = summed(r, i * 64, 64)
            first_full[at, own_columns(t)] = (tok_full[at, own_columns(t)].astype(F32) + total).astype(BF16)

    def norm_rows(source, gain, r):
        size = 32

        @pl.loop(0, rows // size)
        def _(i):
            at = pl.ds(pl.multiple_of(r * rows + i * size, size), size)
            values = source[at, :].astype(F32)
            scale = lax.rsqrt(jnp.sum(values * values, axis=1, keepdims=True) / width + 1e-06)
            normed[at, :] = (values * scale * gain[...]).astype(BF16)

    channels = w0.shape[1]
    block = w3.shape[1]
    units = w4.shape[1]
    tap_count = taps_ref.shape[0]

    def mixer(r):
        for w in range(3):
            weight = full[w][...].reshape(width, channels)
            proj[w] = jnp.dot(normed[set_rows(r), :], weight, preferred_element_type=F32).astype(BF16)
        taps = taps_ref[:, pl.ds(pl.multiple_of(t * channels, 128), channels)]

        @pl.loop(0, seqs)
        def _(i):
            at = pl.ds(pl.multiple_of(i * length, length), length)
            product = proj[1, at, :].astype(F32) * proj[2, at, :].astype(F32)
            position = lax.broadcasted_iota(jnp.int32, product.shape, 0)
            conv = jnp.zeros_like(product)
            for offset in range(tap_count):
                shift = tap_count - 1 - offset
                moved = product if shift == 0 else jnp.where(position >= shift, pltpu.roll(product, shift, 0), 0.0)
                conv = conv + taps[offset : offset + 1, :] * moved
            gated[at, :] = (proj[0, at, :].astype(F32) * conv).astype(BF16)

        @pl.loop(0, n)
        def _(b):
            at = pl.ds(pl.multiple_of(b * block, 128), block)
            part[set_rows(r), at] = jnp.dot(gated[...], full[3][b], preferred_element_type=F32).astype(BF16)

    def hidden_tile(r, start, size):
        at = pl.ds(start, size)
        left = normed[set_rows(r), :]
        gate = jnp.dot(left, full[GATE][:, :, at].reshape(width, size), preferred_element_type=F32)
        upward = jnp.dot(left, full[UP][:, :, at].reshape(width, size), preferred_element_type=F32)
        hidden[set_rows(r), at] = (gate / (1.0 + jnp.exp(-gate)) * upward).astype(BF16)

    def hidden_rows(r):
        @pl.loop(0, units // 256)
        def _(j):
            hidden_tile(r, pl.multiple_of(j * 256, 256), 256)

        if units % 256:
            hidden_tile(r, units // 256 * 256, units % 256)

    wide = w6.shape[1]
    piece = wide // chunk_counts[DOWN]
    per_owner = columns // piece

    def down_to_pair(r, k, slot, start):
        inside = pl.ds(pl.multiple_of(slot * piece, 128), piece)
        return pltpu.make_async_remote_copy(
            src_ref=part.at[set_rows(r), pl.ds(start, piece)], dst_ref=pair_recv.at[r, k, :, inside],
            send_sem=down_pair_ss.at[r, k, slot], recv_sem=down_pair_rs.at[r, k, slot],
            device_id={"tp": pair}, device_id_type=MESH,
        )

    def down_to_far(r, k, slot, start):
        inside = pl.ds(pl.multiple_of(slot * piece, 128), piece)
        return pltpu.make_async_remote_copy(
            src_ref=part.at[set_rows(r), pl.ds(start, piece)], dst_ref=far_recv.at[r, k, :, inside],
            send_sem=down_far_ss.at[r, k, slot], recv_sem=down_far_rs.at[r, k, slot],
            device_id={"tp": lax.rem(t + 2 * k, n_tp)}, device_id_type=MESH,
        )

    def down_strip(c):
        @pl.loop(0, 3)
        def _(phase):
            @pl.loop(0, n)
            def _(b):
                start = pl.multiple_of(b * wide + c * piece, 128)
                owner = (b * wide + c * piece) // columns
                slot = lax.rem((b * wide + c * piece) // piece, per_owner)
                k = lax.rem(owner // 2 - t // 2 + chips, chips)
                other = lax.rem(owner + t, 2)
                mine = (1 - other) * (2 - lax.min(k, 1))

                @pl.when(mine == phase)
                def _():
                    down_piece(b, c, start, slot, k, other)

    def down_piece(b, c, start, slot, k, other):
        part[:, pl.ds(start, piece)] = jnp.dot(
            hidden[...], full[DOWN][b, :, strip(c)], preferred_element_type=F32
        ).astype(BF16)

        @pl.when(other == 1)
        def _():
            for r in (1, 0):
                down_to_pair(r, k, slot, start).start()

        @pl.when((other == 0) & (k > 0))
        def _():
            for r in (1, 0):
                down_to_pair(r, k, slot, start).wait_recv()
                inside = pl.ds(pl.multiple_of(slot * piece, 128), piece)

                @pl.loop(0, rows // 64)
                def _(i):
                    here = pl.ds(pl.multiple_of(i * 64, 64), 64)
                    at = pl.ds(pl.multiple_of(r * rows + i * 64, 64), 64)
                    both = part[at, pl.ds(start, piece)].astype(F32) + pair_recv[r, k, here, inside].astype(F32)
                    part[at, pl.ds(start, piece)] = both.astype(BF16)

                down_to_far(r, k, slot, start).start()

    def square_copy(r, k, peer):
        return pltpu.make_async_remote_copy(
            src_ref=sq_send.at[r], dst_ref=sq_recv.at[r, k - 1], send_sem=sq_ss.at[r, k - 1],
            recv_sem=sq_rs.at[r, k - 1], device_id={"tp": peer}, device_id_type=MESH,
        )

    def squares_send(r):
        for slot in range(per_owner):
            down_to_pair(r, 0, slot, 0).wait_recv()
            for k in range(1, chips):
                down_to_far(r, k, slot, 0).wait_recv()

        @pl.loop(0, seqs)
        def _(i):
            at, total = summed(r, i * length, length)
            second = first_full[at, own_columns(t)].astype(F32) + total
            squares = jnp.sum(second * second, axis=1, keepdims=True)
            sq_send[r, i] = jnp.transpose(jnp.broadcast_to(squares, (length, length)))[:8, :]

        for k in range(1, n_tp):
            square_copy(r, k, lax.rem(t + k, n_tp)).start()

    def close(r, dst):
        for k in range(1, n_tp):
            square_copy(r, k, lax.rem(t + n_tp - k, n_tp)).wait_recv()
        gain = out_gain[:, own_columns(t)]

        @pl.loop(0, seqs)
        def _(i):
            at, total = summed(r, i * length, length)
            second = first_full[at, own_columns(t)].astype(F32) + total
            squares = sq_send[r, i]
            for k in range(1, n_tp):
                squares = squares + sq_recv[r, k - 1, i]
            factor = column(lax.rsqrt(squares[:1, :] / width + 1e-06))
            inside = pl.ds(pl.multiple_of(i * length, length), length)
            dst[inside, :] = (second * factor * gain).astype(BF16)

    guest = lax.select(f == 1, 0, n - 1)
    has_guest = (f == 1) | (f == n - 2)
    inner = lax.select(f == 0, 1, n - 2)

    def tokens_in(device):
        return pltpu.make_async_remote_copy(
            src_ref=tok_ref, dst_ref=block_of(tok_full, 1, t), send_sem=guest_sem.at[0], recv_sem=guest_sem.at[1],
            device_id={"fs": device}, device_id_type=MESH,
        )

    def result_out(device):
        return pltpu.make_async_remote_copy(
            src_ref=returned, dst_ref=returned, send_sem=guest_sem.at[2], recv_sem=guest_sem.at[3],
            device_id={"fs": device}, device_id_type=MESH,
        )

    @pl.when(jnp.logical_not(is_host))
    def _():
        def halves(w, wait):
            @pl.loop(0, chunk_counts[w])
            def _(c):
                for k in range(1, parts):
                    if wait:
                        other_half(w, c, k).wait_send()
                    else:
                        other_half(w, c, k).start()

        tokens_in(inner).start()
        for w in range(MIXER):
            start_own(w)
        for w in range(SHARED, MIXER):
            halves(w, False)
        for w in (GATE, UP):
            start_own(w)
            halves(w, False)

        @pl.loop(0, chunk_counts[DOWN])
        def _(c):
            start_chunk(DOWN, c)
            for k in range(1, parts):
                other_half(DOWN, c, k).start()

        tokens_in(inner).wait_send()
        for w in range(7):
            if w >= SHARED:
                halves(w, True)

            @pl.loop(0, chunk_counts[w])
            def _(c):
                src = own_region(w, g, c)

                @pl.when(f == 0)
                def _():
                    z_copy(w, c, f, src, 1).wait_send()

                @pl.when(f == n - 1)
                def _():
                    z_copy(w, c, f, src, -1).wait_send()

        result_out(inner).wait_recv()
        out_ref[...] = returned[...]

    @pl.when(is_host)
    def _():
        own_tokens = pltpu.make_async_copy(tok_ref, block_of(tok_full, 0, t), own_sem.at[7])
        own_tokens.start()
        for w in range(MIXER):
            start_own(w)
        for w in range(7):
            own_copy(w).start()
        own_tokens.wait()
        gather_send(tok_full, 0, 0)
        steps = range(n - 2)
        for s in steps:
            receive(0, s)

        @pl.when(has_guest)
        def _():
            tokens_in(guest).wait_recv()

        gather_send(tok_full, 0, 1)
        gather_relay(tok_full, 0, 0)
        for w in range(1, MIXER):
            for s in steps:
                receive(w, s)
        start_own(GATE)
        gather_finish(tok_full, 0, 0)
        norm_rows(tok_full, mix_gain, 0)
        for w in range(MIXER):
            own_copy(w).wait()
            for s in steps:
                finish(w, s)
        mixer(0)
        sum_send(0)
        gather_relay(tok_full, 0, 1)
        receive(GATE, 0)
        start_own(UP)
        gather_finish(tok_full, 0, 1)
        norm_rows(tok_full, mix_gain, 1)
        sum_relay(0)
        mixer(1)
        sum_send(1)
        first_rows(0)
        gather_send(first_full, 2, 0)
        sum_relay(1)
        for s in steps[1:]:
            receive(GATE, s)
        receive(UP, 0)
        start_own(DOWN)
        gather_relay(first_full, 2, 0)
        first_rows(1)
        gather_send(first_full, 2, 1)
        gather_finish(first_full, 2, 0)
        norm_rows(first_full, ffn_gain, 0)
        for s in steps[1:]:
            receive(UP, s)
        gather_relay(first_full, 2, 1)
        for w in (GATE, UP):
            own_copy(w).wait()
            for s in steps:
                finish(w, s)
        hidden_rows(0)
        for s in steps:
            receive_chunk(DOWN, s, 0)
        gather_finish(first_full, 2, 1)
        norm_rows(first_full, ffn_gain, 1)
        hidden_rows(1)
        for r in range(2):
            for k in range(chips):
                to_pair(r, k).wait_send()
            for k in range(1, chips):
                to_far(r, k).wait_send()
        own_copy(DOWN).wait()

        @pl.loop(0, chunk_counts[DOWN])
        def _(c):
            @pl.when(c > 0)
            def _():
                for s in steps:
                    receive_chunk(DOWN, s, c)

            for s in steps:
                finish_chunk(DOWN, s, c)
            down_strip(c)

        squares_send(1)
        squares_send(0)
        close(1, returned)

        @pl.when(has_guest)
        def _():
            result_out(guest).start()

        close(0, out_ref)

        @pl.when(has_guest)
        def _():
            result_out(guest).wait_send()

        for r in range(2):
            gather_sent(tok_full, 0, r)
            gather_sent(first_full, 2, r)
            for k in range(1, n_tp):
                square_copy(r, k, lax.rem(t + k, n_tp)).wait_send()
            for slot in range(per_owner):
                for k in range(chips):
                    down_to_pair(r, k, slot, 0).wait_send()
                for k in range(1, chips):
                    down_to_far(r, k, slot, 0).wait_send()
        for w in range(7):
            @pl.loop(0, chunk_counts[w])
            def _(c):
                @pl.loop(0, n)
                def _(blk):
                    here = region(w, blk, g, c)

                    @pl.when((f + 1 <= last_host) & (blk <= f))
                    def _():
                        z_copy(w, c, blk, here, 1).wait_send()

                    @pl.when((f - 1 >= first_host) & (blk >= f))
                    def _():
                        z_copy(w, c, blk, here, -1).wait_send()

                    whole = ((blk == 0) & (f == 1)) | ((blk == n - 1) & (f == n - 2))
                    if w < SHARED:
                        whole = blk == f

                    @pl.when((blk != f) & jnp.logical_not(whole))
                    def _():
                        for k in range(1, parts):
                            y_copy(w, c, blk, g, k, y_peer(k)).wait_send()


def solution(mesh):
    n, parts, n_tp = mesh.shape["fs"], mesh.shape["grp"], mesh.shape["tp"]

    def local(tokens, mix_gain, outer, inner, value, taps, mix_out, ffn_gain, gate, up, down, out_gain):
        seqs, length, columns = tokens.shape
        rows, width = seqs * length, columns * n_tp
        weights = (outer, inner, value, mix_out, gate, up, down)
        counts = tuple(1 if w < MIXER else chunks_of(a.shape[0] // parts) for w, a in enumerate(weights))
        wide = down.shape[1]
        strips = next(count for count in (4, 2, 1) if wide % (count * 128) == 0 or count == 1)
        counts = counts[:-1] + (strips,)
        slots = sum(counts)
        channels, units = outer.shape[1], gate.shape[1]
        others, y_others = max(n_tp - 1, 1), max(parts - 1, 1)
        per_owner = columns * strips // wide
        dma = pltpu.SemaphoreType.DMA
        scratch = [pltpu.VMEM((n,) + a.shape, BF16) for a in weights]
        chips = n_tp // 2
        scratch += [
            pltpu.VMEM((2 * rows, width), BF16),
            pltpu.VMEM((2 * rows, width), BF16),
            pltpu.VMEM((3, rows, channels), BF16),
            pltpu.VMEM((rows, channels), BF16),
            pltpu.VMEM((2 * rows, width), BF16),
            pltpu.VMEM((2, chips, rows, columns), BF16),
            pltpu.VMEM((2, chips, rows, columns), BF16),
            pltpu.VMEM((2 * rows, width), BF16),
            pltpu.VMEM((2 * rows, units), BF16),
            pltpu.VMEM((rows, columns), BF16),
            pltpu.VMEM((2, seqs, 8, length), F32),
            pltpu.VMEM((2, others, seqs, 8, length), F32),
            dma((slots, n)), dma((slots, n)), dma((slots, n)),
            dma((slots, n, y_others)), dma((slots, n, y_others)),
            dma((8,)), dma((3, 2, chips)), dma((3, 2, chips)), dma((3, 2, chips)), dma((3, 2, chips)),
            dma((2, chips, per_owner)), dma((2, chips, per_owner)),
            dma((2, chips, per_owner)), dma((2, chips, per_owner)),
            dma((2, others)), dma((2, others)), dma((4,)),
        ]
        out = pl.pallas_call(
            functools.partial(kernel, n, parts, n_tp, length, counts),
            out_shape=jax.ShapeDtypeStruct((rows, columns), BF16),
            in_specs=[pl.BlockSpec(memory_space=pltpu.VMEM)] * 12,
            out_specs=pl.BlockSpec(memory_space=pltpu.VMEM),
            scratch_shapes=scratch,
            compiler_params=pltpu.CompilerParams(
                collective_id=0, has_side_effects=True, vmem_limit_bytes=62 * 1024 * 1024
            ),
        )(
            tokens.reshape(rows, columns), mix_gain[None], outer, inner, value, taps, mix_out,
            ffn_gain[None], gate, up, down, out_gain[None],
        )
        return out.reshape(seqs, length, columns)

    in_specs = (
        P(("grp", "fs"), None, "tp"), P(), P("fs", "tp"), P("fs", "tp"), P("fs", "tp"), P(), P("tp", "fs"),
        P(), P("fs", "tp"), P("fs", "tp"), P("tp", "fs"), P(),
    )
    out_specs = P(("grp", "fs"), None, "tp")
    return jax.shard_map(local, mesh=mesh, in_specs=in_specs, out_specs=out_specs, check_vma=False)
```

```python
import functools

import jax
import jax.numpy as jnp
from jax import lax
from jax.experimental import pallas as pl
from jax.experimental.pallas import tpu as pltpu
from jax.sharding import PartitionSpec as P

MESH = pl.DeviceIdType.MESH
F32 = jnp.float32
BF16 = jnp.bfloat16
MIXER = 4
GATE, UP, DOWN = 4, 5, 6
SHARED = 2


def chunks_of(half):
    return next(count for count in (4, 2, 1) if half % (count * 16) == 0 or count == 1)


def column(rows):
    wide = jnp.broadcast_to(rows, (rows.shape[1], rows.shape[1]))
    return jnp.transpose(wide)[:, :1]


def kernel(
    n, parts, n_tp, length, chunk_counts,
    tok_ref, mix_gain, w0, w1, w2, taps_ref, w3, ffn_gain, w4, w5, w6, out_gain,
    out_ref,
    f0, f1, f2, f3, f4, f5, f6,
    tok_full, normed, proj, gated, part, pair_recv, far_recv, first_full, hidden, returned, sq_send, sq_recv,
    right_send, left_send, z_recv, y_send, y_recv, own_sem, pair_ss, pair_rs, far_ss, far_rs,
    down_pair_ss, down_pair_rs, down_far_ss, down_far_rs, sq_ss, sq_rs, guest_sem,
):
    own = (w0, w1, w2, w3, w4, w5, w6)
    full = (f0, f1, f2, f3, f4, f5, f6)
    f, g, t = lax.axis_index("fs"), lax.axis_index("grp"), lax.axis_index("tp")
    rows, columns = tok_ref.shape
    width = columns * n_tp
    seqs = rows // length
    bases = [sum(chunk_counts[:w]) for w in range(7)]

    def y_peer(k):
        return lax.rem(g + k, parts)

    def tp_peer(k):
        return lax.rem(t + k, n_tp)

    def span(w, half, c):
        size = own[w].shape[0] // parts
        piece = size // chunk_counts[w]
        start = half * size + c * piece
        return pl.ds(pl.multiple_of(start, 8), piece)

    def region(w, blk, half, c):
        return full[w].at[blk, span(w, half, c), :]

    barrier = pltpu.get_barrier_semaphore()
    for k in range(1, n_tp):
        pl.semaphore_signal(barrier, inc=1, device_id={"tp": tp_peer(k)}, device_id_type=MESH)
    for k in range(1, parts):
        pl.semaphore_signal(barrier, inc=1, device_id={"grp": y_peer(k)}, device_id_type=MESH)

    @pl.when(f < n - 1)
    def _():
        pl.semaphore_signal(barrier, inc=1, device_id={"fs": f + 1}, device_id_type=MESH)

    @pl.when(f > 0)
    def _():
        pl.semaphore_signal(barrier, inc=1, device_id={"fs": f - 1}, device_id_type=MESH)

    neighbours = lax.min(f, 1) + lax.min(n - 1 - f, 1)
    pl.semaphore_wait(barrier, n_tp - 1 + parts - 1 + neighbours)

    def z_copy(w, c, blk, src, step):
        send = right_send if step > 0 else left_send
        return pltpu.make_async_remote_copy(
            src_ref=src, dst_ref=region(w, blk, g, c),
            send_sem=send.at[bases[w] + c, blk], recv_sem=z_recv.at[bases[w] + c, blk],
            device_id={"fs": f + step}, device_id_type=MESH,
        )

    def y_copy(w, c, blk, half, k, peer):
        return pltpu.make_async_remote_copy(
            src_ref=region(w, blk, half, c), dst_ref=region(w, blk, half, c),
            send_sem=y_send.at[bases[w] + c, blk, k - 1], recv_sem=y_recv.at[bases[w] + c, blk, k - 1],
            device_id={"grp": peer}, device_id_type=MESH,
        )

    first_host, last_host = 1, n - 2
    is_host = (f >= first_host) & (f <= last_host)

    def start_own(w):
        @pl.loop(0, chunk_counts[w])
        def _(c):
            src = own[w].at[span(w, g, c), :]

            @pl.when(f + 1 <= last_host)
            def _():
                z_copy(w, c, f, src, 1).start()

            @pl.when(f - 1 >= first_host)
            def _():
                z_copy(w, c, f, src, -1).start()

    def other_half(w, c, k):
        half = lax.rem(g + parts - k, parts)
        inward = lax.select(f == 0, 1, n - 2)
        return pltpu.make_async_remote_copy(
            src_ref=own[w].at[span(w, half, c), :], dst_ref=region(w, f, half, c),
            send_sem=y_send.at[bases[w] + c, f, k - 1], recv_sem=y_recv.at[bases[w] + c, f, k - 1],
            device_id={"fs": inward}, device_id_type=MESH,
        )

    def receive(w, s):
        left, right = f - 1 - s, f + 1 + s

        @pl.loop(0, chunk_counts[w])
        def _(c):
            def arrived(blk, step, whole):
                z_copy(w, c, blk, region(w, blk, g, c), -step).wait_recv()
                onward = (f + 1 <= last_host) if step > 0 else (f - 1 >= first_host)

                @pl.when(onward)
                def _():
                    z_copy(w, c, blk, region(w, blk, g, c), step).start()

                def share():
                    for k in range(1, parts):
                        y_copy(w, c, blk, g, k, y_peer(k)).start()

                if s == 0 and w >= SHARED:
                    pl.when(jnp.logical_not(whole))(share)
                else:
                    share()

            @pl.when(right < n)
            def _():
                arrived(right, -1, right == n - 1)

            @pl.when(left >= 0)
            def _():
                arrived(left, 1, left == 0)

    def finish(w, s):
        @pl.loop(0, chunk_counts[w])
        def _(c):
            for k in range(1, parts):
                source = lax.rem(g + parts - k, parts)
                for blk, there in ((f - 1 - s, f - 1 - s >= 0), (f + 1 + s, f + 1 + s < n)):
                    @pl.when(there)
                    def _():
                        y_copy(w, c, blk, source, k, source).wait_recv()

    def own_copy(w):
        return pltpu.make_async_copy(own[w], full[w].at[f], own_sem.at[w])

    def own_columns(owner):
        return pl.ds(pl.multiple_of(owner * columns, 128), columns)

    chips = n_tp // 2
    core = lax.rem(t, 2)
    pair = t + 1 - 2 * core

    def ahead(k, start=None):
        return lax.rem((t if start is None else start) + 2 * k, n_tp)

    def behind(k, start=None):
        return lax.rem((t if start is None else start) + n_tp - 2 * k, n_tp)

    def set_rows(r):
        return pl.ds(r * rows, rows)

    def pair_copy(stage, r, k, src, dst):
        return pltpu.make_async_remote_copy(
            src_ref=src, dst_ref=dst, send_sem=pair_ss.at[stage, r, k], recv_sem=pair_rs.at[stage, r, k],
            device_id={"tp": pair}, device_id_type=MESH,
        )

    def far_copy(stage, r, k, src, dst, peer):
        return pltpu.make_async_remote_copy(
            src_ref=src, dst_ref=dst, send_sem=far_ss.at[stage, r, k], recv_sem=far_rs.at[stage, r, k],
            device_id={"tp": peer}, device_id_type=MESH,
        )

    def block_of(buf, r, owner):
        return buf.at[set_rows(r), own_columns(owner)]

    def gather_send(buf, stage, r):
        mine = block_of(buf, r, t)
        for k in range(1, chips):
            far_copy(stage, r, k, mine, mine, ahead(k)).start()
        pair_copy(stage, r, 0, mine, mine).start()

    def gather_relay(buf, stage, r):
        for k in range(1, chips):
            theirs = block_of(buf, r, behind(k))
            far_copy(stage, r, k, theirs, theirs, behind(k)).wait_recv()
            pair_copy(stage, r, k, theirs, theirs).start()

    def gather_finish(buf, stage, r):
        for k in range(chips):
            theirs = block_of(buf, r, behind(k, pair))
            pair_copy(stage, r, k, theirs, theirs).wait_recv()

    def gather_sent(buf, stage, r):
        mine = block_of(buf, r, t)
        for k in range(1, chips):
            far_copy(stage, r, k, mine, mine, ahead(k)).wait_send()
        for k in range(chips):
            pair_copy(stage, r, k, mine, mine).wait_send()

    def to_pair(r, k):
        return pair_copy(1, r, k, block_of(part, r, ahead(k, pair)), pair_recv.at[r, k])

    def to_far(r, k):
        return far_copy(1, r, k, block_of(part, r, ahead(k)), far_recv.at[r, k], ahead(k))

    def sum_send(r):
        for k in range(chips - 1, -1, -1):
            to_pair(r, k).start()

    def sum_relay(r):
        for k in range(1, chips):
            to_pair(r, k).wait_recv()

            @pl.loop(0, rows // 64)
            def _(i):
                inside = pl.ds(pl.multiple_of(i * 64, 64), 64)
                at = pl.ds(pl.multiple_of(r * rows + i * 64, 64), 64)
                both = part[at, own_columns(ahead(k))].astype(F32) + pair_recv[r, k, inside, :].astype(F32)
                part[at, own_columns(ahead(k))] = both.astype(BF16)

            to_far(r, k).start()

    def summed(r, start, size):
        inside = pl.ds(pl.multiple_of(start, size), size)
        at = pl.ds(pl.multiple_of(r * rows + start, size), size)
        total = part[at, own_columns(t)].astype(F32) + pair_recv[r, 0, inside, :].astype(F32)
        for k in range(1, chips):
            total = total + far_recv[r, k, inside, :].astype(F32)
        return at, total

    def first_rows(r):
        to_pair(r, 0).wait_recv()
        for k in range(1, chips):
            to_far(r, k).wait_recv()

        @pl.loop(0, rows // 64)
        def _(i):
            at, total = summed(r, i * 64, 64)
            first_full[at, own_columns(t)] = (tok_full[at, own_columns(t)].astype(F32) + total).astype(BF16)

    def norm_rows(source, gain, r):
        size = 32

        @pl.loop(0, rows // size)
        def _(i):
            at = pl.ds(pl.multiple_of(r * rows + i * size, size), size)
            values = source[at, :].astype(F32)
            scale = lax.rsqrt(jnp.sum(values * values, axis=1, keepdims=True) / width + 1e-06)
            normed[at, :] = (values * scale * gain[...]).astype(BF16)

    channels = w0.shape[1]
    block = w3.shape[1]
    units = w4.shape[1]
    tap_count = taps_ref.shape[0]

    def mixer(r):
        for w in range(3):
            weight = full[w][...].reshape(width, channels)
            proj[w] = jnp.dot(normed[set_rows(r), :], weight, preferred_element_type=F32).astype(BF16)
        taps = taps_ref[:, pl.ds(pl.multiple_of(t * channels, 128), channels)]

        @pl.loop(0, seqs)
        def _(i):
            at = pl.ds(pl.multiple_of(i * length, length), length)
            product = proj[1, at, :].astype(F32) * proj[2, at, :].astype(F32)
            position = lax.broadcasted_iota(jnp.int32, product.shape, 0)
            conv = jnp.zeros_like(product)
            for offset in range(tap_count):
                shift = tap_count - 1 - offset
                moved = product if shift == 0 else jnp.where(position >= shift, pltpu.roll(product, shift, 0), 0.0)
                conv = conv + taps[offset : offset + 1, :] * moved
            gated[at, :] = (proj[0, at, :].astype(F32) * conv).astype(BF16)

        @pl.loop(0, n)
        def _(b):
            at = pl.ds(pl.multiple_of(b * block, 128), block)
            part[set_rows(r), at] = jnp.dot(gated[...], full[3][b], preferred_element_type=F32).astype(BF16)

    def hidden_tile(r, start, size):
        at = pl.ds(start, size)
        left = normed[set_rows(r), :]
        gate = jnp.dot(left, full[GATE][:, :, at].reshape(width, size), preferred_element_type=F32)
        upward = jnp.dot(left, full[UP][:, :, at].reshape(width, size), preferred_element_type=F32)
        hidden[set_rows(r), at] = (gate / (1.0 + jnp.exp(-gate)) * upward).astype(BF16)

    def hidden_rows(r):
        @pl.loop(0, units // 256)
        def _(j):
            hidden_tile(r, pl.multiple_of(j * 256, 256), 256)

        if units % 256:
            hidden_tile(r, units // 256 * 256, units % 256)

    wide = w6.shape[1]
    piece = min(wide, columns)
    per_block, per_owner = wide // piece, columns // piece

    def down_to_pair(r, k, slot, start):
        inside = pl.ds(pl.multiple_of(slot * piece, 128), piece)
        return pltpu.make_async_remote_copy(
            src_ref=part.at[set_rows(r), pl.ds(start, piece)], dst_ref=pair_recv.at[r, k, :, inside],
            send_sem=down_pair_ss.at[r, k, slot], recv_sem=down_pair_rs.at[r, k, slot],
            device_id={"tp": pair}, device_id_type=MESH,
        )

    def down_to_far(r, k, slot, start):
        inside = pl.ds(pl.multiple_of(slot * piece, 128), piece)
        return pltpu.make_async_remote_copy(
            src_ref=part.at[set_rows(r), pl.ds(start, piece)], dst_ref=far_recv.at[r, k, :, inside],
            send_sem=down_far_ss.at[r, k, slot], recv_sem=down_far_rs.at[r, k, slot],
            device_id={"tp": lax.rem(t + 2 * k, n_tp)}, device_id_type=MESH,
        )

    def down_block(b):
        for p in range(per_block):
            start = pl.multiple_of(b * wide + p * piece, 128)
            owner = (b * wide + p * piece) // columns
            slot = lax.rem(b * per_block + p, per_owner)
            k = lax.rem(owner // 2 - t // 2 + chips, chips)
            lane = lax.rem(owner, 2) == core

            @pl.loop(0, 2)
            def _(turn):
                r = 1 - turn
                at = pl.ds(pl.multiple_of(r * rows, rows), rows)
                weight = full[DOWN][b][:, p * piece : (p + 1) * piece]
                part[at, pl.ds(start, piece)] = jnp.dot(
                    hidden[at, :], weight, preferred_element_type=F32
                ).astype(BF16)

                @pl.when(jnp.logical_not(lane))
                def _():
                    down_to_pair(r, k, slot, start).start()

            @pl.when(lane & (k > 0))
            def _():
                for r in (1, 0):
                    down_to_pair(r, k, slot, start).wait_recv()
                    inside = pl.ds(pl.multiple_of(slot * piece, 128), piece)

                    @pl.loop(0, rows // 64)
                    def _(i):
                        here = pl.ds(pl.multiple_of(i * 64, 64), 64)
                        at = pl.ds(pl.multiple_of(r * rows + i * 64, 64), 64)
                        both = part[at, pl.ds(start, piece)].astype(F32) + pair_recv[r, k, here, inside].astype(F32)
                        part[at, pl.ds(start, piece)] = both.astype(BF16)

                    down_to_far(r, k, slot, start).start()

    def square_copy(r, k, peer):
        return pltpu.make_async_remote_copy(
            src_ref=sq_send.at[r], dst_ref=sq_recv.at[r, k - 1], send_sem=sq_ss.at[r, k - 1],
            recv_sem=sq_rs.at[r, k - 1], device_id={"tp": peer}, device_id_type=MESH,
        )

    def squares_send(r):
        for slot in range(per_owner):
            down_to_pair(r, 0, slot, 0).wait_recv()
            for k in range(1, chips):
                down_to_far(r, k, slot, 0).wait_recv()

        @pl.loop(0, seqs)
        def _(i):
            at, total = summed(r, i * length, length)
            second = first_full[at, own_columns(t)].astype(F32) + total
            squares = jnp.sum(second * second, axis=1, keepdims=True)
            sq_send[r, i] = jnp.transpose(jnp.broadcast_to(squares, (length, length)))[:8, :]

        for k in range(1, n_tp):
            square_copy(r, k, lax.rem(t + k, n_tp)).start()

    def close(r, dst):
        for k in range(1, n_tp):
            square_copy(r, k, lax.rem(t + n_tp - k, n_tp)).wait_recv()
        gain = out_gain[:, own_columns(t)]

        @pl.loop(0, seqs)
        def _(i):
            at, total = summed(r, i * length, length)
            second = first_full[at, own_columns(t)].astype(F32) + total
            squares = sq_send[r, i]
            for k in range(1, n_tp):
                squares = squares + sq_recv[r, k - 1, i]
            factor = column(lax.rsqrt(squares[:1, :] / width + 1e-06))
            inside = pl.ds(pl.multiple_of(i * length, length), length)
            dst[inside, :] = (second * factor * gain).astype(BF16)

    guest = lax.select(f == 1, 0, n - 1)
    has_guest = (f == 1) | (f == n - 2)
    inner = lax.select(f == 0, 1, n - 2)

    def tokens_in(device):
        return pltpu.make_async_remote_copy(
            src_ref=tok_ref, dst_ref=block_of(tok_full, 1, t), send_sem=guest_sem.at[0], recv_sem=guest_sem.at[1],
            device_id={"fs": device}, device_id_type=MESH,
        )

    def result_out(device):
        return pltpu.make_async_remote_copy(
            src_ref=returned, dst_ref=returned, send_sem=guest_sem.at[2], recv_sem=guest_sem.at[3],
            device_id={"fs": device}, device_id_type=MESH,
        )

    @pl.when(jnp.logical_not(is_host))
    def _():
        def halves(w, wait):
            @pl.loop(0, chunk_counts[w])
            def _(c):
                for k in range(1, parts):
                    if wait:
                        other_half(w, c, k).wait_send()
                    else:
                        other_half(w, c, k).start()

        tokens_in(inner).start()
        for w in range(MIXER):
            start_own(w)
        for w in range(SHARED, MIXER):
            halves(w, False)
        for w in range(MIXER, 7):
            start_own(w)
            halves(w, False)
        tokens_in(inner).wait_send()
        for w in range(7):
            if w >= SHARED:
                halves(w, True)

            @pl.loop(0, chunk_counts[w])
            def _(c):
                src = own[w].at[span(w, g, c), :]

                @pl.when(f == 0)
                def _():
                    z_copy(w, c, f, src, 1).wait_send()

                @pl.when(f == n - 1)
                def _():
                    z_copy(w, c, f, src, -1).wait_send()

        result_out(inner).wait_recv()
        out_ref[...] = returned[...]

    @pl.when(is_host)
    def _():
        own_tokens = pltpu.make_async_copy(tok_ref, block_of(tok_full, 0, t), own_sem.at[7])
        own_tokens.start()
        for w in range(MIXER):
            start_own(w)
        for w in range(7):
            own_copy(w).start()
        own_tokens.wait()
        gather_send(tok_full, 0, 0)
        steps = range(n - 2)
        for s in steps:
            receive(0, s)

        @pl.when(has_guest)
        def _():
            tokens_in(guest).wait_recv()

        gather_send(tok_full, 0, 1)
        gather_relay(tok_full, 0, 0)
        for w in range(1, MIXER):
            for s in steps:
                receive(w, s)
        start_own(GATE)
        gather_finish(tok_full, 0, 0)
        norm_rows(tok_full, mix_gain, 0)
        for w in range(MIXER):
            own_copy(w).wait()
            for s in steps:
                finish(w, s)
        mixer(0)
        sum_send(0)
        gather_relay(tok_full, 0, 1)
        receive(GATE, 0)
        start_own(UP)
        gather_finish(tok_full, 0, 1)
        norm_rows(tok_full, mix_gain, 1)
        sum_relay(0)
        mixer(1)
        sum_send(1)
        first_rows(0)
        gather_send(first_full, 2, 0)
        sum_relay(1)
        for s in steps[1:]:
            receive(GATE, s)
        receive(UP, 0)
        start_own(DOWN)
        gather_relay(first_full, 2, 0)
        first_rows(1)
        gather_send(first_full, 2, 1)
        gather_finish(first_full, 2, 0)
        norm_rows(first_full, ffn_gain, 0)
        for s in steps[1:]:
            receive(UP, s)
        gather_relay(first_full, 2, 1)
        for w in (GATE, UP):
            own_copy(w).wait()
            for s in steps:
                finish(w, s)
        hidden_rows(0)
        receive(DOWN, 0)
        gather_finish(first_full, 2, 1)
        norm_rows(first_full, ffn_gain, 1)
        hidden_rows(1)
        for r in range(2):
            for k in range(chips):
                to_pair(r, k).wait_send()
            for k in range(1, chips):
                to_far(r, k).wait_send()
        own_copy(DOWN).wait()
        down_block(f)

        for s in steps:
            if s > 0:
                receive(DOWN, s)
            finish(DOWN, s)

            @pl.loop(0, 2)
            def _(side):
                b = lax.select(side == 0, f - 1 - s, f + 1 + s)

                @pl.when((b >= 0) & (b < n))
                def _():
                    down_block(b)

        squares_send(1)
        squares_send(0)
        close(1, returned)

        @pl.when(has_guest)
        def _():
            result_out(guest).start()

        close(0, out_ref)

        @pl.when(has_guest)
        def _():
            result_out(guest).wait_send()

        for r in range(2):
            gather_sent(tok_full, 0, r)
            gather_sent(first_full, 2, r)
            for k in range(1, n_tp):
                square_copy(r, k, lax.rem(t + k, n_tp)).wait_send()
            for slot in range(per_owner):
                for k in range(chips):
                    down_to_pair(r, k, slot, 0).wait_send()
                for k in range(1, chips):
                    down_to_far(r, k, slot, 0).wait_send()
        for w in range(7):
            @pl.loop(0, chunk_counts[w])
            def _(c):
                @pl.loop(0, n)
                def _(blk):
                    here = region(w, blk, g, c)

                    @pl.when((f + 1 <= last_host) & (blk <= f))
                    def _():
                        z_copy(w, c, blk, here, 1).wait_send()

                    @pl.when((f - 1 >= first_host) & (blk >= f))
                    def _():
                        z_copy(w, c, blk, here, -1).wait_send()

                    whole = ((blk == 0) & (f == 1)) | ((blk == n - 1) & (f == n - 2))
                    if w < SHARED:
                        whole = blk == f

                    @pl.when((blk != f) & jnp.logical_not(whole))
                    def _():
                        for k in range(1, parts):
                            y_copy(w, c, blk, g, k, y_peer(k)).wait_send()


def solution(mesh):
    n, parts, n_tp = mesh.shape["fs"], mesh.shape["grp"], mesh.shape["tp"]

    def local(tokens, mix_gain, outer, inner, value, taps, mix_out, ffn_gain, gate, up, down, out_gain):
        seqs, length, columns = tokens.shape
        rows, width = seqs * length, columns * n_tp
        weights = (outer, inner, value, mix_out, gate, up, down)
        counts = tuple(1 if w < MIXER else chunks_of(a.shape[0] // parts) for w, a in enumerate(weights))
        slots = sum(counts)
        channels, units = outer.shape[1], gate.shape[1]
        others, y_others = max(n_tp - 1, 1), max(parts - 1, 1)
        per_owner = columns // min(down.shape[1], columns)
        dma = pltpu.SemaphoreType.DMA
        scratch = [pltpu.VMEM((n,) + a.shape, BF16) for a in weights]
        chips = n_tp // 2
        scratch += [
            pltpu.VMEM((2 * rows, width), BF16),
            pltpu.VMEM((2 * rows, width), BF16),
            pltpu.VMEM((3, rows, channels), BF16),
            pltpu.VMEM((rows, channels), BF16),
            pltpu.VMEM((2 * rows, width), BF16),
            pltpu.VMEM((2, chips, rows, columns), BF16),
            pltpu.VMEM((2, chips, rows, columns), BF16),
            pltpu.VMEM((2 * rows, width), BF16),
            pltpu.VMEM((2 * rows, units), BF16),
            pltpu.VMEM((rows, columns), BF16),
            pltpu.VMEM((2, seqs, 8, length), F32),
            pltpu.VMEM((2, others, seqs, 8, length), F32),
            dma((slots, n)), dma((slots, n)), dma((slots, n)),
            dma((slots, n, y_others)), dma((slots, n, y_others)),
            dma((8,)), dma((3, 2, chips)), dma((3, 2, chips)), dma((3, 2, chips)), dma((3, 2, chips)),
            dma((2, chips, per_owner)), dma((2, chips, per_owner)),
            dma((2, chips, per_owner)), dma((2, chips, per_owner)),
            dma((2, others)), dma((2, others)), dma((4,)),
        ]
        out = pl.pallas_call(
            functools.partial(kernel, n, parts, n_tp, length, counts),
            out_shape=jax.ShapeDtypeStruct((rows, columns), BF16),
            in_specs=[pl.BlockSpec(memory_space=pltpu.VMEM)] * 12,
            out_specs=pl.BlockSpec(memory_space=pltpu.VMEM),
            scratch_shapes=scratch,
            compiler_params=pltpu.CompilerParams(
                collective_id=0, has_side_effects=True, vmem_limit_bytes=62 * 1024 * 1024
            ),
        )(
            tokens.reshape(rows, columns), mix_gain[None], outer, inner, value, taps, mix_out,
            ffn_gain[None], gate, up, down, out_gain[None],
        )
        return out.reshape(seqs, length, columns)

    in_specs = (
        P(("grp", "fs"), None, "tp"), P(), P("fs", "tp"), P("fs", "tp"), P("fs", "tp"), P(), P("tp", "fs"),
        P(), P("fs", "tp"), P("fs", "tp"), P("tp", "fs"), P(),
    )
    out_specs = P(("grp", "fs"), None, "tp")
    return jax.shard_map(local, mesh=mesh, in_specs=in_specs, out_specs=out_specs, check_vma=False)
```
